32 devices in a mesh: sp: 16 (over z, y, core), tp: 2 (over x).
Axes of the slice: x: 2, y: 2, z: 4, core: 2. Of those that a mesh axis runs over, the one named last changes fastest.
Arguments:
- asking_matrix: bfloat16 [2048, 2048], P('sp', 'tp'), may hold values from -30 to 30
- matching_key_matrix: bfloat16 [2048, 1024], P('sp', 'tp'), may hold values from -30 to 30
- carried_value_matrix: bfloat16 [2048, 1024], P('sp', 'tp'), may hold values from -48 to 48
- silu_switch_argument: bfloat16 [2048, 2048], P('sp', 'tp'), may hold values from -6 to 6
- duality_source_matrix: bfloat16 [2048, 2048], P('sp', 'tp'), may hold values from -6 to 6
- storing_direction_matrix: bfloat16 [2048, 1024], P('sp', 'tp'), may hold values from -6 to 6
- fetching_direction_matrix: bfloat16 [2048, 1024], P('sp', 'tp'), may hold values from -6 to 6
- duality_kernel_coefficients: bfloat16 [5, 2048], P(None, 'tp'), may hold values from -2.5 to 2.5
- storing_kernel_coefficients: bfloat16 [5, 1024], P(None, 'tp'), may hold values from -2.5 to 2.5
- fetching_kernel_coefficients: bfloat16 [5, 1024], P(None, 'tp'), may hold values from -2.5 to 2.5
- raw_increment_lengths: float32 [2, 32, 2048], P(None, 'tp', 'sp'), may hold values from -5.5 to 5.5
- logarithmic_fading_speeds: float32 [2, 32], P(None, 'tp'), may hold values from -16 to -2.9
- token_fading_spikes: float32 [2, 32, 2048], P(None, 'tp', 'sp'), may hold values from -2.1 to 0
- absorber_score_vector: float32 [16], P('tp'), may hold values from 4 to 8
- cluster_scaling_factor: float32 [2048], P('tp'), may hold values from 0.1 to 1.9
- final_mapping_matrix: bfloat16 [2, 2048, 4096], P(None, 'tp', 'sp'), may hold values from -0.09375 to 0.09375
Outputs:
- mixed_out: bfloat16 [2048, 4096], P(('sp', 'tp'))
The draws below stay inside these ranges and needn't reach their ends.
All inputs are finite; a program needn't handle non-finite values.
Results may differ from the reference program's by a relative error of at most 0.014.
Values may be sent and summed in bfloat16 or wider, within the bound.
No kernel may reach another device: no remote copies, remote signals or barrier semaphores. Data moves between devices by JAX's collectives and lax.ppermute only.
A program may use at most 128 MiB of HBM per device.

```python
import math
import jax
import jax.numpy as jnp
from jax import lax

D = 4096
HEADS = 16
KV_HEADS = 8
HEAD = 128
SSD_HEADS = 32
SSD_HEAD = 64
GROUPS = 8
STATE = 128
CONV = 5
WINDOW = 128
SPAN = 128
TOK_DEV = 128
TOKENS = 2048
ATTN_W = 2048
KV_W = 1024
SSD_W = 2048
N_TP = 2


def drawn_rows(key):
    query_base = jnp.clip(jax.random.normal(jax.random.fold_in(key, 11), (TOKENS, ATTN_W), jnp.float32), -4.0, 4.0)
    key_base = jnp.clip(jax.random.normal(jax.random.fold_in(key, 12), (TOKENS, KV_W), jnp.float32), -4.0, 4.0)
    return (query_base, key_base)


def draw_asking_matrix(key, part):
    return drawn_rows(key)[0].astype(jnp.bfloat16)


def draw_matching_key_matrix(key, part):
    return drawn_rows(key)[1].astype(jnp.bfloat16)


def draw_raw_increment_lengths(key, part):
    jitter = jnp.clip(jax.random.normal(jax.random.fold_in(key, 21), (2, SSD_HEADS, TOKENS), jnp.float32), -4.0, 4.0)
    block_level = jax.random.uniform(jax.random.fold_in(key, 22), (2, SSD_HEADS, TOKENS // TOK_DEV), jnp.float32, -1.5, 1.5)
    return jitter + jnp.repeat(block_level, TOK_DEV, axis=2)


def draw_logarithmic_fading_speeds(key, part):
    keep_count = SSD_HEADS // 2
    ranking = jnp.stack([jax.random.permutation(jax.random.fold_in(key, 31), SSD_HEADS), jax.random.permutation(jax.random.fold_in(key, 32), SSD_HEADS)])
    lasting = ranking < keep_count
    slow_rate = jnp.exp(jax.random.uniform(jax.random.fold_in(key, 33), (2, SSD_HEADS), jnp.float32, math.log(0.02), math.log(0.3))) / TOKENS
    fast_rate = jnp.exp(jax.random.uniform(jax.random.fold_in(key, 34), (2, SSD_HEADS), jnp.float32, math.log(1.0 / 70.0), math.log(1.0 / 20.0)))
    return jnp.log(jnp.where(lasting, slow_rate, fast_rate))


def draw_token_fading_spikes(key, part):
    positions = jax.random.randint(jax.random.fold_in(key, 41), (2, SSD_HEADS, 3), 0, TOKENS)
    depths = jax.random.uniform(jax.random.fold_in(key, 42), (2, SSD_HEADS, 3), jnp.float32, 0.22, 0.69)
    places = jnp.arange(TOKENS, dtype=jnp.int32)
    hits = jnp.where(places[None, None, None, :] == positions[..., None], depths[..., None], 0.0)
    return -jnp.sum(hits, axis=2)


def block_levels(rng, dims, shards, smallest, top_value):
    loudness, own = 1.0, jax.random.fold_in(rng, 6)
    for position, blocks in shards:
        heights = jnp.exp(jax.random.uniform(jax.random.fold_in(own, position), (blocks,), jnp.float32, smallest / len(shards), top_value / len(shards)))
        loudness = loudness * jnp.repeat(heights, dims[position] // blocks).reshape([-1 if axis == position else 1 for axis in range(len(dims))])
    return loudness


def noise(stream_key, shape, scale, most, split=(), held_as=jnp.bfloat16):
    gain = block_levels(stream_key, shape, split, -0.22, 0.18) if split else 1.0
    values = jax.random.normal(stream_key, shape, jnp.float32) * scale * gain
    return jnp.minimum(jnp.maximum(values, -most), most).astype(held_as)


def setup_inputs(seed: int = 0) -> dict:
    key_of = jax.random.split(jax.random.key(seed), 17)
    asking_matrix = draw_asking_matrix(jax.random.fold_in(key_of[16], 71), 0)
    matching_key_matrix = draw_matching_key_matrix(jax.random.fold_in(key_of[16], 71), 0)
    carried_value_matrix = noise(key_of[2], (TOKENS, KV_W), 8.0, 48.0, ((0, 16), (1, 2)))
    silu_switch_argument = noise(key_of[3], (TOKENS, SSD_W), 1.0, 6.0, ((0, 16), (1, 2)))
    duality_source_matrix = noise(key_of[4], (TOKENS, SSD_W), 1.0, 6.0, ((0, 16), (1, 2)))
    storing_direction_matrix = noise(key_of[5], (TOKENS, GROUPS * STATE), 1.0, 6.0, ((0, 16), (1, 2)))
    fetching_direction_matrix = noise(key_of[6], (TOKENS, GROUPS * STATE), 1.0, 6.0, ((0, 16), (1, 2)))
    duality_kernel_coefficients = noise(key_of[7], (CONV, SSD_W), CONV ** -0.5, 2.5, ((1, 2),))
    storing_kernel_coefficients = noise(key_of[8], (CONV, GROUPS * STATE), CONV ** -0.5, 2.5, ((1, 2),))
    fetching_kernel_coefficients = noise(key_of[9], (CONV, GROUPS * STATE), CONV ** -0.5, 2.5, ((1, 2),))
    raw_increment_lengths = draw_raw_increment_lengths(jax.random.fold_in(key_of[16], 71), 0)
    logarithmic_fading_speeds = draw_logarithmic_fading_speeds(jax.random.fold_in(key_of[16], 71), 0)
    token_fading_spikes = draw_token_fading_spikes(jax.random.fold_in(key_of[16], 71), 0)
    absorber_score_vector = jnp.clip(4.0 + 4.0 * jax.random.uniform(key_of[13], (HEADS,), jnp.float32) ** block_levels(key_of[13], (HEADS,), ((0, 2),), -0.2, 0.2), 4.0, 8.0)
    cluster_scaling_factor = jnp.clip(1.0 + 0.18 * jax.random.normal(key_of[14], (SSD_W,), jnp.float32), 0.1, 1.9)
    final_mapping_matrix = noise(key_of[15], (2, ATTN_W, D), (2 * ATTN_W) ** -0.5, 0.09375, ((1, 2), (2, 16)))
    return {"asking_matrix": asking_matrix, "matching_key_matrix": matching_key_matrix, "carried_value_matrix": carried_value_matrix, "silu_switch_argument": silu_switch_argument, "duality_source_matrix": duality_source_matrix, "storing_direction_matrix": storing_direction_matrix, "fetching_direction_matrix": fetching_direction_matrix, "duality_kernel_coefficients": duality_kernel_coefficients, "storing_kernel_coefficients": storing_kernel_coefficients, "fetching_kernel_coefficients": fetching_kernel_coefficients, "raw_increment_lengths": raw_increment_lengths, "logarithmic_fading_speeds": logarithmic_fading_speeds, "token_fading_spikes": token_fading_spikes, "absorber_score_vector": absorber_score_vector, "cluster_scaling_factor": cluster_scaling_factor, "final_mapping_matrix": final_mapping_matrix}


ROTARY_BASE = 500000.0
EPSILON = 1e-06

def rotate(matrix, offset):
    row_count = matrix.shape[0]
    halfway = HEAD // 2
    heads_here = matrix.shape[1] // HEAD
    spacing = ROTARY_BASE ** (-jnp.arange(halfway, dtype=jnp.float32) * 2.0 / HEAD)
    places = (offset + jnp.arange(row_count, dtype=jnp.int32)).astype(jnp.float32)
    angles = places[:, None] * spacing[None, :]
    cosine = jnp.cos(angles)[:, None, :]
    sine_table = jnp.sin(angles)[:, None, :]
    halves = matrix.astype(jnp.float32).reshape(row_count, heads_here, 2, halfway)
    former = halves[:, :, 0]
    latter = halves[:, :, 1]
    turned = jnp.stack([former * cosine - latter * sine_table, latter * cosine + former * sine_table], axis=2)
    return turned.reshape(row_count, heads_here * HEAD).astype(jnp.bfloat16)

def attend(turned_queries, turned_keys, carried_value_matrix, absorber_score_vector):
    sharing = HEADS // KV_HEADS
    block_count = TOKENS // SPAN
    filler = jnp.zeros((SPAN, KV_W), jnp.bfloat16)
    key_pad = jnp.concatenate([filler, turned_keys, filler], axis=0)
    value_pad = jnp.concatenate([filler, carried_value_matrix, filler], axis=0)
    within = jnp.arange(SPAN, dtype=jnp.int32)[:, None]
    across = jnp.arange(3 * SPAN, dtype=jnp.int32)[None, :]
    inside = jnp.abs(across - SPAN - within) <= WINDOW
    sink_rows = absorber_score_vector.reshape(KV_HEADS, sharing)[:, :, None, None]

    def one_block(block_index):
        first_row = (block_index * SPAN).astype(jnp.int32)
        query_tile = lax.dynamic_slice_in_dim(turned_queries, first_row, SPAN, 0).reshape(SPAN, KV_HEADS, sharing, HEAD)
        key_tile = lax.dynamic_slice_in_dim(key_pad, first_row, 3 * SPAN, 0).reshape(3 * SPAN, KV_HEADS, HEAD)
        value_tile = lax.dynamic_slice_in_dim(value_pad, first_row, 3 * SPAN, 0).reshape(3 * SPAN, KV_HEADS, HEAD)
        places = first_row - SPAN + across
        allowed = inside & (places >= 0) & (places < TOKENS)
        scores = jnp.einsum('qkgd,skd->kgqs', query_tile.astype(jnp.float32), key_tile.astype(jnp.float32)) * HEAD ** (-0.5)
        scores = jnp.where(allowed, scores, -jnp.inf)
        ceiling = jnp.maximum(lax.optimization_barrier(jnp.max(scores, axis=-1, keepdims=True)), sink_rows)
        weights = jnp.exp(scores - ceiling)
        denominator = lax.optimization_barrier(jnp.sum(weights, axis=-1, keepdims=True)) + jnp.exp(sink_rows - ceiling)
        probabilities = (weights / denominator).astype(jnp.bfloat16)
        attended = jnp.einsum('kgqs,skd->qkgd', probabilities.astype(jnp.float32), value_tile.astype(jnp.float32))
        return attended.reshape(SPAN, ATTN_W).astype(jnp.bfloat16)
    return lax.map(one_block, jnp.arange(block_count, dtype=jnp.int32)).reshape(TOKENS, ATTN_W)

def convolve(padded, taps_all, row_count):
    summed = jnp.zeros((row_count, padded.shape[1]), jnp.float32)
    for tap_index in range(CONV):
        summed = summed + padded[tap_index:tap_index + row_count].astype(jnp.float32) * taps_all[tap_index].astype(jnp.float32)
    return jax.nn.silu(summed).astype(jnp.bfloat16)

def sweep(scan_rows, step_rows, decay_rows, write_rows, read_rows):
    per_group = SSD_HEADS // GROUPS
    block_count = TOKENS // SPAN
    highest = lax.Precision.HIGHEST
    scan_tiles = scan_rows.reshape(block_count, SPAN, GROUPS, per_group, SSD_HEAD)
    step_tiles = step_rows.reshape(block_count, SPAN, GROUPS, per_group)
    decay_tiles = decay_rows.reshape(block_count, SPAN, GROUPS, per_group)
    write_tiles = write_rows.reshape(block_count, SPAN, GROUPS, STATE)
    read_tiles = read_rows.reshape(block_count, SPAN, GROUPS, STATE)
    earlier_mask = jnp.arange(SPAN)[:, None] >= jnp.arange(SPAN)[None, :]

    def advance(carried, block_item):
        scan_tile, step_tile, decay_tile, write_tile, read_tile = block_item
        scaled = scan_tile.astype(jnp.float32) * step_tile[..., None]
        write_values = write_tile.astype(jnp.float32)
        read_values = read_tile.astype(jnp.float32)
        running = jnp.cumsum(decay_tile, axis=0)
        spread = running[:, None] - running[None, :]
        fading = jnp.exp(jnp.where(earlier_mask[:, :, None, None], spread, -jnp.inf))
        affinity = jnp.einsum('lgn,sgn->lsg', read_values, write_values, precision=highest)
        within_block = jnp.einsum('lsgr,sgrp->lgrp', affinity[..., None] * fading, scaled, precision=highest)
        from_before = jnp.einsum('lgn,grpn->lgrp', read_values, carried, precision=highest) * jnp.exp(running)[..., None]
        to_end = jnp.exp(running[-1:] - running)
        block_states = jnp.einsum('lgn,lgrp->grpn', write_values, scaled * to_end[..., None], precision=highest)
        return (carried * jnp.exp(running[-1])[..., None, None] + block_states, within_block + from_before)
    start_state = jnp.zeros((GROUPS, per_group, SSD_HEAD, STATE), jnp.float32)
    final_state, outputs = lax.scan(advance, start_state, (scan_tiles, step_tiles, decay_tiles, write_tiles, read_tiles))
    return outputs.reshape(TOKENS, SSD_W)

def reference(asking_matrix, matching_key_matrix, carried_value_matrix, silu_switch_argument, duality_source_matrix, storing_direction_matrix, fetching_direction_matrix, duality_kernel_coefficients, storing_kernel_coefficients, fetching_kernel_coefficients, raw_increment_lengths, logarithmic_fading_speeds, token_fading_spikes, absorber_score_vector, cluster_scaling_factor, final_mapping_matrix):
    attended = attend(rotate(asking_matrix, 0), rotate(matching_key_matrix, 0), carried_value_matrix, absorber_score_vector)
    margin = CONV // 2
    raw_rows = jnp.concatenate([duality_source_matrix, storing_direction_matrix, fetching_direction_matrix], axis=1)
    padded = jnp.pad(raw_rows, ((margin, margin), (0, 0)))
    conved = convolve(padded, jnp.concatenate([duality_kernel_coefficients, storing_kernel_coefficients, fetching_kernel_coefficients], axis=1), TOKENS)
    per_group = SSD_HEADS // GROUPS
    scan_rows = conved[:, :SSD_W].reshape(TOKENS, GROUPS, per_group, SSD_HEAD)
    write_rows = conved[:, SSD_W:SSD_W + GROUPS * STATE].reshape(TOKENS, GROUPS, STATE)
    read_rows = conved[:, SSD_W + GROUPS * STATE:].reshape(TOKENS, GROUPS, STATE)
    joint_increment_lengths = jax.nn.softplus(raw_increment_lengths)
    joint_fading_amounts = -jnp.exp(logarithmic_fading_speeds)[:, :, None] * joint_increment_lengths + token_fading_spikes
    steps_rows = jnp.transpose(joint_increment_lengths, (0, 2, 1)).reshape(2, TOKENS, GROUPS, per_group)
    decay_rows = jnp.transpose(joint_fading_amounts, (0, 2, 1)).reshape(2, TOKENS, GROUPS, per_group)
    ahead_rows = sweep(scan_rows, steps_rows[0], decay_rows[0], write_rows, read_rows)
    back_rows = sweep(scan_rows[::-1], steps_rows[1][::-1], decay_rows[1][::-1], write_rows[::-1], read_rows[::-1])[::-1]
    gated_rows = (ahead_rows + back_rows) * jax.nn.silu(silu_switch_argument.astype(jnp.float32))
    grouped = gated_rows.reshape(TOKENS, GROUPS, SSD_W // GROUPS)
    grouped = grouped * lax.rsqrt(lax.optimization_barrier(jnp.mean(grouped * grouped, axis=-1, keepdims=True)) + EPSILON)
    normed = (grouped.reshape(TOKENS, SSD_W) * cluster_scaling_factor).astype(jnp.bfloat16)
    slice_width = ATTN_W // N_TP
    summed = jnp.zeros((TOKENS, D), jnp.float32)
    for shard_index in range(N_TP):
        first_col = shard_index * slice_width
        partial_sum = jnp.dot(attended[:, first_col:first_col + slice_width], final_mapping_matrix[0, first_col:first_col + slice_width], preferred_element_type=jnp.float32)
        partial_sum = partial_sum + jnp.dot(normed[:, first_col:first_col + slice_width], final_mapping_matrix[1, first_col:first_col + slice_width], preferred_element_type=jnp.float32)
        rounded = lax.optimization_barrier(partial_sum.astype(jnp.bfloat16))
        summed = summed + rounded.astype(jnp.float32)
    return summed.astype(jnp.bfloat16)
```

```python
import functools

import jax
import jax.numpy as jnp
from jax import lax
from jax.experimental import pallas as pl
from jax.experimental.pallas import tpu as pltpu
from jax.sharding import PartitionSpec as P

HEAD = 128
SSD_HEAD = 64
STATE = 128
CONV = 5
WINDOW = 128
EDGE = 16

ROTARY_BASE = 500000.0
EPSILON = 1e-06
HIGHEST = lax.Precision.HIGHEST
F32 = jnp.float32
BF16 = jnp.bfloat16
VMEM = pl.BlockSpec(memory_space=pltpu.VMEM)
SMEM = pl.BlockSpec(memory_space=pltpu.SMEM)


def call(kernel, outs, ins, flops, scratch=(), scalars=1, name=None):
    moved = sum(a.size * a.dtype.itemsize for a in list(ins) + list(outs))
    return pl.pallas_call(
        kernel,
        out_shape=outs,
        in_specs=[SMEM] * scalars + [VMEM] * (len(ins) - scalars),
        out_specs=[VMEM] * len(outs),
        scratch_shapes=list(scratch),
        cost_estimate=pl.CostEstimate(flops=flops, bytes_accessed=moved, transcendentals=0),
        name=name,
    )(*ins)


def nn(a, b, precision=None):
    return lax.dot_general(
        a, b, (((1,), (0,)), ((), ())), precision=precision, preferred_element_type=F32
    )


def nt(a, b, precision=None):
    return lax.dot_general(
        a, b, (((1,), (1,)), ((), ())), precision=precision, preferred_element_type=F32
    )


def silu(v):
    return v / (1.0 + jnp.exp(-v))


def head_spread(heads, cols):
    head = lax.broadcasted_iota(jnp.int32, (heads, cols), 0)
    col = lax.broadcasted_iota(jnp.int32, (heads, cols), 1)
    return jnp.where(col // SSD_HEAD == head, 1.0, 0.0).astype(F32)


def block_kernel(
    place,
    x_ref,
    w_ref,
    r_ref,
    prev_ref,
    next_ref,
    tx_ref,
    tw_ref,
    tr_ref,
    inc_ref,
    fade_ref,
    spike_ref,
    keep_ref,
    send_ref,
    read_ref,
    y_ref,
    expl_ref,
    line,
    xs,
    ws,
):
    rows, cols = x_ref.shape
    wide = w_ref.shape[1]
    heads = cols // SSD_HEAD
    groups = wide // STATE
    per = heads // groups
    margin = CONV // 2
    start = 0
    for src, taps, dst in ((x_ref, tx_ref, xs), (w_ref, tw_ref, ws), (r_ref, tr_ref, read_ref)):
        span = src.shape[1]
        line[0:EDGE, 0:span] = prev_ref[:, start : start + span].astype(F32)
        line[EDGE : EDGE + rows, 0:span] = src[...].astype(F32)
        line[EDGE + rows : 2 * EDGE + rows, 0:span] = next_ref[:, start : start + span].astype(F32)
        step = min(span, 256)
        for at in range(0, span, step):
            total = jnp.zeros((rows, step), F32)
            for k in range(CONV):
                low = EDGE - margin + k
                total = total + line[low : low + rows, at : at + step] * taps[
                    k : k + 1, at : at + step
                ].astype(F32)
            dst[:, at : at + step] = silu(total).astype(BF16)
        start += span

    steps = jax.nn.softplus(inc_ref[...])
    logs = -jnp.exp(fade_ref[...]) * steps + spike_ref[...]
    first = lax.broadcasted_iota(jnp.int32, (rows, rows), 0)
    second = lax.broadcasted_iota(jnp.int32, (rows, rows), 1)
    lower = first >= second
    upper = first <= second
    run_f = nn(logs[0:heads], jnp.where(upper, 1.0, 0.0), HIGHEST)
    run_b = nn(logs[heads : 2 * heads], jnp.where(lower, 1.0, 0.0), HIGHEST)
    tall = jnp.concatenate([run_f, run_b], axis=0).T
    expl_ref[...] = jnp.exp(tall)
    tot_f = run_f[:, rows - 1 : rows]
    tot_b = run_b[:, 0:1]
    end_f = jnp.exp(tot_f - run_f) * steps[0:heads]
    end_b = jnp.exp(tot_b - run_b) * steps[heads : 2 * heads]

    spread = head_spread(heads, cols)
    tot = jnp.exp(jnp.concatenate([tall[rows - 1 : rows, 0:heads], tall[0:1, heads:]], axis=0))
    tot = nn(tot, spread, HIGHEST)
    high = tot.astype(BF16)
    low = (tot - high.astype(F32)).astype(BF16)
    half = cols // 2
    tail = jnp.concatenate(
        [high.astype(F32), low.astype(F32), jnp.zeros((EDGE - 4, cols), F32)], axis=0
    ).astype(BF16)
    for side in range(2):
        part = tail[:, side * half : (side + 1) * half]

        @pl.when(place[0] == side)
        def _():
            keep_ref[2 * STATE : 2 * STATE + EDGE, :] = part

        @pl.when(place[0] != side)
        def _():
            send_ref[2 * STATE : 2 * STATE + EDGE, :] = part

    for g in range(groups):
        wg = ws[:, g * STATE : (g + 1) * STATE]
        rg = read_ref[:, g * STATE : (g + 1) * STATE]
        affinity = nt(rg, wg)
        turned = wg.astype(F32).T
        fresh = []
        for j in range(per):
            h = g * per + j
            at = h * SSD_HEAD
            ahead = jnp.exp(
                jnp.where(lower, tall[:, h : h + 1] - run_f[h : h + 1, :], -jnp.inf)
            ) * steps[h : h + 1, :]
            back = jnp.exp(
                jnp.where(
                    upper, tall[:, heads + h : heads + h + 1] - run_b[h : h + 1, :], -jnp.inf
                )
            ) * steps[heads + h : heads + h + 1, :]
            mixed = (affinity * (ahead + back)).astype(BF16)
            grow_f = (turned * end_f[h : h + 1, :]).astype(BF16)
            grow_b = (turned * end_b[h : h + 1, :]).astype(BF16)
            got = nn(jnp.concatenate([mixed, grow_f, grow_b], axis=0), xs[:, at : at + SSD_HEAD])
            y_ref[:, at : at + SSD_HEAD] = got[0:rows]
            fresh.append(got[rows : rows + 2 * STATE].astype(BF16))
        whole = jnp.concatenate(fresh, axis=1)
        size = per * SSD_HEAD
        base = g * size
        for side in range(2):
            a = max(base, side * half)
            b = min(base + size, (side + 1) * half)
            if a >= b:
                continue
            part = whole[:, a - base : b - base]

            @pl.when(place[0] == side)
            def _():
                keep_ref[0 : 2 * STATE, a - side * half : b - side * half] = part

            @pl.when(place[0] != side)
            def _():
                send_ref[0 : 2 * STATE, a - side * half : b - side * half] = part


def attend_kernel(
    place, sink, q_ref, k_ref, v_ref, prev_ref, next_ref, cos_ref, sin_ref, out_ref
):
    rows = q_ref.shape[0]
    kv = k_ref.shape[1] // HEAD
    sharing = q_ref.shape[1] // k_ref.shape[1]
    wide = k_ref.shape[1]

    def turn(m, low):
        m = m.astype(F32)
        half = HEAD // 2
        other = jnp.concatenate([m[:, half:], m[:, :half]], axis=1)
        high = low + m.shape[0]
        return (m * cos_ref[low:high, :] + other * sin_ref[low:high, :]).astype(BF16)

    within = lax.broadcasted_iota(jnp.int32, (rows, 3 * rows), 0)
    across = lax.broadcasted_iota(jnp.int32, (rows, 3 * rows), 1)
    far = across - rows - within
    allowed = (far <= WINDOW) & (far >= -WINDOW)
    allowed = allowed & ((across >= rows) | (place[0] > 0))
    allowed = allowed & ((across < 2 * rows) | (place[0] < place[1] - 1))
    for g in range(kv):
        at = g * HEAD
        keys = jnp.concatenate(
            [
                turn(prev_ref[:, at : at + HEAD], 0),
                turn(k_ref[:, at : at + HEAD], rows),
                turn(next_ref[:, at : at + HEAD], 2 * rows),
            ],
            axis=0,
        )
        values = jnp.concatenate(
            [
                prev_ref[:, wide + at : wide + at + HEAD],
                v_ref[:, at : at + HEAD],
                next_ref[:, wide + at : wide + at + HEAD],
            ],
            axis=0,
        )
        for j in range(sharing):
            h = g * sharing + j
            query = turn(q_ref[:, h * HEAD : (h + 1) * HEAD], rows)
            scores = nt(query, keys) * HEAD ** (-0.5)
            scores = jnp.where(allowed, scores, -jnp.inf)
            top = jnp.maximum(jnp.max(scores, axis=1, keepdims=True), sink[h])
            weights = jnp.exp(scores - top)
            total = jnp.sum(weights, axis=1, keepdims=True) + jnp.exp(sink[h] - top)
            chance = (weights / total).astype(BF16)
            out_ref[:, h * HEAD : (h + 1) * HEAD] = nn(chance, values).astype(BF16)


def finish_kernel(place, y_ref, read_ref, expl_ref, own_ref, got_ref, gate_ref, gain_ref, out_ref):
    rows, cols = y_ref.shape
    wide = read_ref.shape[1]
    heads = cols // SSD_HEAD
    groups = wide // STATE
    size = cols // groups
    half = cols // 2
    spread = head_spread(heads, cols)
    for g in range(groups):
        at = g * size
        rg = read_ref[:, g * STATE : (g + 1) * STATE]
        pieces = []
        for low in range(at, at + size, min(size, half)):
            span = min(size, half)
            side = low // half
            off = low - side * half
            mine = place[0] == side
            pieces.append(
                jnp.where(
                    mine,
                    own_ref[:, off : off + span].astype(F32),
                    got_ref[:, off : off + span].astype(F32),
                ).astype(BF16)
            )
        states = pieces[0] if len(pieces) == 1 else jnp.concatenate(pieces, axis=1)
        local = spread[:, at : at + size]
        fade_f = nn(expl_ref[:, 0:heads], local, HIGHEST)
        fade_b = nn(expl_ref[:, heads : 2 * heads], local, HIGHEST)
        both = (
            y_ref[:, at : at + size]
            + fade_f * nn(rg, states[0:STATE])
            + fade_b * nn(rg, states[STATE : 2 * STATE])
        )
        gated = both * silu(gate_ref[:, at : at + size].astype(F32))
        mean = jnp.sum(gated * gated, axis=1, keepdims=True) * (1.0 / size)
        out_ref[:, at : at + size] = (
            gated * lax.rsqrt(mean + EPSILON) * gain_ref[:, at : at + size]
        ).astype(BF16)


def project_kernel(count, place, a_ref, ap_ref, n_ref, np_ref, *refs):
    shards = refs[:count]
    own_ref, x_ref, c_ref, cx_ref = refs[count:]
    rows = a_ref.shape[0]
    half = rows // 2
    left = jnp.concatenate([a_ref[...], ap_ref[...]], axis=0)
    right = jnp.concatenate([n_ref[...], np_ref[...]], axis=0)
    for j in range(count):
        span = shards[j].shape[2]
        at = j * span
        total = (nn(left, shards[j][0]) + nn(right, shards[j][1])).astype(BF16)
        for side in range(2):

            @pl.when(place[0] == side)
            def _():
                a, b = side * half, (1 - side) * half
                own_ref[:, at : at + span] = total[a : a + half]
                x_ref[:, at : at + span] = total[b : b + half]
                c_ref[:, at : at + span] = total[rows + a : rows + a + half]
                cx_ref[:, at : at + span] = total[rows + b : rows + b + half]


def place_kernel(masks, spans, place, *refs):
    out_ref = refs[-1]
    for i, group in enumerate(masks):
        own, x, c, cx = refs[4 * i : 4 * i + 4]
        span = spans
        for j, _ in enumerate(group):
            index = sum(len(m) for m in masks[:i]) + j
            at = j * span
            mine = pl.multiple_of(place[2 * index] * span, span)
            theirs = pl.multiple_of(place[2 * index + 1] * span, span)
            out_ref[:, pl.ds(mine, span)] = (
                own[:, at : at + span].astype(F32) + x[:, at : at + span].astype(F32)
            ).astype(BF16)
            out_ref[:, pl.ds(theirs, span)] = (
                c[:, at : at + span].astype(F32) + cx[:, at : at + span].astype(F32)
            ).astype(BF16)


def flip(a, count, mask):
    return lax.ppermute(a, "sp", [(i, i ^ mask) for i in range(count)])


def shift(a, count, by):
    return lax.ppermute(
        a, "sp", [(i, i + by) for i in range(count) if 0 <= i + by < count]
    )


def exchange_states(keep, send, count, me):
    half = keep.shape[1]
    core = me & 1
    got = flip(send, count, 1)

    def split(a):
        tail = a[2 * STATE :].astype(F32)
        return (
            a[:STATE].astype(F32),
            a[STATE : 2 * STATE].astype(F32),
            tail[0:1] + tail[2:3],
            tail[1:2] + tail[3:4],
        )

    mine = split(keep)
    theirs = split(got)
    pick = lambda flag, a, b: jax.tree.map(lambda u, v: jnp.where(flag, u, v), a, b)
    low = pick(core == 0, mine, theirs)
    high = pick(core == 0, theirs, mine)
    join = lambda low, high: (
        low[0] * high[2] + high[0],
        high[1] * low[3] + low[1],
        low[2] * high[2],
        low[3] * high[3],
    )
    pair = (low, high)
    total = join(low, high)
    into_f = jnp.zeros((STATE, half), F32)
    into_b = jnp.zeros((STATE, half), F32)
    gap_f = jnp.ones((1, half), F32)
    gap_b = jnp.ones((1, half), F32)
    bit = 2
    while bit < count:
        upper = (me & bit) != 0
        last = bit * 2 >= count
        if last:
            payload = jnp.where(upper, total[1], total[0]).astype(BF16)
            other = flip(payload, count, bit).astype(F32)
            into_f = jnp.where(upper, other * gap_f + into_f, into_f)
            into_b = jnp.where(upper, into_b, other * gap_b + into_b)
        else:
            fades = jnp.concatenate([total[2], total[3]], axis=0)
            top = fades.astype(BF16)
            rest = (fades - top.astype(F32)).astype(BF16)
            payload = jnp.concatenate(
                [
                    total[0].astype(BF16),
                    total[1].astype(BF16),
                    top,
                    rest,
                    jnp.zeros((EDGE - 4, half), BF16),
                ],
                axis=0,
            )
            other = split(flip(payload, count, bit))
            low = pick(upper, other, total)
            high = pick(upper, total, other)
            into_f = jnp.where(upper, other[0] * gap_f + into_f, into_f)
            into_b = jnp.where(upper, into_b, other[1] * gap_b + into_b)
            gap_f = jnp.where(upper, gap_f * other[2], gap_f)
            gap_b = jnp.where(upper, gap_b, gap_b * other[3])
            total = join(low, high)
        bit *= 2
    low, high = pair
    first = jnp.concatenate([into_f, into_b * high[3] + high[1]], axis=0).astype(BF16)
    second = jnp.concatenate([into_f * low[2] + low[0], into_b], axis=0).astype(BF16)
    own = jnp.where(core == 0, first, second)
    away = jnp.where(core == 0, second, first)
    return own, flip(away, count, 1)


def local(
    asking_matrix,
    matching_key_matrix,
    carried_value_matrix,
    silu_switch_argument,
    duality_source_matrix,
    storing_direction_matrix,
    fetching_direction_matrix,
    duality_kernel_coefficients,
    storing_kernel_coefficients,
    fetching_kernel_coefficients,
    raw_increment_lengths,
    logarithmic_fading_speeds,
    token_fading_spikes,
    absorber_score_vector,
    cluster_scaling_factor,
    final_mapping_matrix,
):
    rows = asking_matrix.shape[0]
    me = lax.axis_index("sp")
    side = lax.axis_index("tp")
    count = lax.axis_size("sp")
    tps = lax.axis_size("tp")
    cols = duality_source_matrix.shape[1]
    wide = storing_direction_matrix.shape[1]
    heads = cols // SSD_HEAD
    core = (me & 1).astype(jnp.int32).reshape(1)
    sds = jax.ShapeDtypeStruct

    raw = (duality_source_matrix, storing_direction_matrix, fetching_direction_matrix)
    tail = jnp.concatenate([a[rows - EDGE :] for a in raw], axis=1)
    lead = jnp.concatenate([a[:EDGE] for a in raw], axis=1)
    prev_edge = shift(tail, count, 1)
    next_edge = shift(lead, count, -1)
    pairs = jnp.concatenate([matching_key_matrix, carried_value_matrix], axis=1)
    prev_pair = shift(pairs, count, 1)
    next_pair = shift(pairs, count, -1)

    shards = {0: final_mapping_matrix}
    bits = []
    bit = count // 2
    while bit >= 2:
        bits.append(bit)
        bit //= 2
    for bit in bits:
        for mask in list(shards):
            shards[mask ^ bit] = flip(shards[mask], count, bit)

    keep, send, read, inner, expl = call(
        block_kernel,
        [
            sds((2 * STATE + EDGE, cols // 2), BF16),
            sds((2 * STATE + EDGE, cols // 2), BF16),
            sds((rows, wide), BF16),
            sds((rows, cols), F32),
            sds((rows, 2 * heads), F32),
        ],
        [
            core,
            *raw,
            prev_edge,
            next_edge,
            duality_kernel_coefficients,
            storing_kernel_coefficients,
            fetching_kernel_coefficients,
            raw_increment_lengths.reshape(2 * heads, rows),
            logarithmic_fading_speeds.reshape(2 * heads, 1),
            token_fading_spikes.reshape(2 * heads, rows),
        ],
        flops=4 * 10**9,
        scratch=[
            pltpu.VMEM((rows + 2 * EDGE, max(cols, wide)), F32),
            pltpu.VMEM((rows, cols), BF16),
            pltpu.VMEM((rows, wide), BF16),
        ],
        name="block",
    )
    own_state, got_state = exchange_states(keep, send, count, me)

    halfway = HEAD // 2
    spacing = ROTARY_BASE ** (-jnp.arange(halfway, dtype=F32) * 2.0 / HEAD)
    places = ((me - 1) * rows + jnp.arange(3 * rows, dtype=jnp.int32)).astype(F32)
    angles = places[:, None] * spacing[None, :]
    cosine = jnp.cos(angles)
    sine = jnp.sin(angles)
    cosine = jnp.concatenate([cosine, cosine], axis=1)
    sine = jnp.concatenate([-sine, sine], axis=1)
    where = jnp.stack([me, jnp.int32(count)]).astype(jnp.int32)
    (attended,) = call(
        attend_kernel,
        [sds(asking_matrix.shape, BF16)],
        [
            where,
            absorber_score_vector,
            asking_matrix,
            matching_key_matrix,
            carried_value_matrix,
            prev_pair,
            next_pair,
            cosine,
            sine,
        ],
        flops=3 * 10**9,
        scalars=2,
        name="attend",
    )
    attended_pair = flip(attended, count, 1)

    (normed,) = call(
        finish_kernel,
        [sds((rows, cols), BF16)],
        [
            core,
            inner,
            read,
            expl,
            own_state,
            got_state,
            silu_switch_argument,
            cluster_scaling_factor.reshape(1, cols),
        ],
        flops=3 * 10**9,
        name="finish",
    )
    normed_pair = flip(normed, count, 1)

    masks = list(shards)
    span = final_mapping_matrix.shape[2]
    if tps == 2 and span % 128 == 0:
        cut = len(masks) - max(1, len(masks) // 4)
        groups = [masks[:cut], masks[cut:]]
        pieces = []
        diag = [(2 * i + j, 2 * (i ^ 1) + 1 - j) for i in range(count) for j in range(2)]
        for group in groups:
            width = span * len(group)
            outs = call(
                functools.partial(project_kernel, len(group)),
                [sds((rows // 2, width), BF16)] * 4,
                [
                    side.astype(jnp.int32).reshape(1),
                    attended,
                    attended_pair,
                    normed,
                    normed_pair,
                    *[shards[m] for m in group],
                ],
                flops=4 * 10**8 * len(group),
                name="project",
            )
            pieces += [
                outs[0],
                lax.ppermute(outs[1], "tp", [(0, 1), (1, 0)]),
                flip(outs[2], count, 1),
                lax.ppermute(outs[3], ("sp", "tp"), diag),
            ]
        order = []
        for m in masks:
            order += [me ^ m, me ^ 1 ^ m]
        (out,) = call(
            functools.partial(place_kernel, groups, span),
            [sds((rows // 2, span * count), BF16)],
            [jnp.stack(order).astype(jnp.int32), *pieces],
            flops=10**6,
            name="place",
        )
        return out

    left = jnp.concatenate(
        [
            jnp.concatenate([attended, normed], axis=1),
            jnp.concatenate([attended_pair, normed_pair], axis=1),
        ],
        axis=0,
    )
    stacked = jnp.concatenate([shards[m] for m in masks], axis=2).reshape(
        -1, span * len(masks)
    )
    partial = jnp.dot(left, stacked, preferred_element_type=F32).astype(BF16)
    partial = partial.reshape(2, tps, rows // tps, -1)
    summed = lax.psum_scatter(partial, "tp", scatter_dimension=1, tiled=True)
    summed = summed.reshape(2, rows // tps, len(masks), span)
    own, away = summed[0], flip(summed[1], count, 1)
    full = [None] * count
    for j, m in enumerate(masks):
        full[m] = own[:, j]
        full[m ^ 1] = away[:, j]
    full = jnp.stack(full, axis=0)
    bit = 1
    while bit < count:
        seen = full.reshape(count // (2 * bit), 2, bit, rows // tps, span)
        full = jnp.where((me & bit) != 0, seen[:, ::-1], seen).reshape(full.shape)
        bit *= 2
    return jnp.moveaxis(full, 0, 1).reshape(rows // tps, count * span)


def solution(mesh):
    in_specs = (
        P("sp", "tp"),
        P("sp", "tp"),
        P("sp", "tp"),
        P("sp", "tp"),
        P("sp", "tp"),
        P("sp", "tp"),
        P("sp", "tp"),
        P(None, "tp"),
        P(None, "tp"),
        P(None, "tp"),
        P(None, "tp", "sp"),
        P(None, "tp"),
        P(None, "tp", "sp"),
        P("tp"),
        P("tp"),
        P(None, "tp", "sp"),
    )
    out_specs = P(("sp", "tp"), None)
    return jax.shard_map(local, mesh=mesh, in_specs=in_specs, out_specs=out_specs, check_vma=False)
```

```python
import functools

import jax
import jax.numpy as jnp
from jax import lax
from jax.experimental import pallas as pl
from jax.experimental.pallas import tpu as pltpu
from jax.sharding import PartitionSpec as P


HEAD = 128
SSD_HEAD = 64
STATE = 128
CONV = 5
WINDOW = 128
EDGE = 16

ROTARY_BASE = 500000.0
EPSILON = 1e-06
HIGHEST = lax.Precision.HIGHEST
F32 = jnp.float32
BF16 = jnp.bfloat16
VMEM = pl.BlockSpec(memory_space=pltpu.VMEM)
SMEM = pl.BlockSpec(memory_space=pltpu.SMEM)


def call(kernel, outs, ins, flops, scratch=(), scalars=1):
    moved = sum(a.size * a.dtype.itemsize for a in list(ins) + list(outs))
    return pl.pallas_call(
        kernel,
        out_shape=outs,
        in_specs=[SMEM] * scalars + [VMEM] * (len(ins) - scalars),
        out_specs=[VMEM] * len(outs),
        scratch_shapes=list(scratch),
        cost_estimate=pl.CostEstimate(flops=flops, bytes_accessed=moved, transcendentals=0),
    )(*ins)


def nn(a, b, precision=None):
    return lax.dot_general(
        a, b, (((1,), (0,)), ((), ())), precision=precision, preferred_element_type=F32
    )


def nt(a, b, precision=None):
    return lax.dot_general(
        a, b, (((1,), (1,)), ((), ())), precision=precision, preferred_element_type=F32
    )


def silu(v):
    return v / (1.0 + jnp.exp(-v))


def head_spread(heads, cols):
    head = lax.broadcasted_iota(jnp.int32, (heads, cols), 0)
    col = lax.broadcasted_iota(jnp.int32, (heads, cols), 1)
    return jnp.where(col // SSD_HEAD == head, 1.0, 0.0).astype(F32)


def block_kernel(
    place,
    x_ref,
    w_ref,
    r_ref,
    prev_ref,
    next_ref,
    tx_ref,
    tw_ref,
    tr_ref,
    inc_ref,
    fade_ref,
    spike_ref,
    keep_ref,
    send_ref,
    read_ref,
    y_ref,
    expl_ref,
    line,
    xs,
    ws,
):
    rows, cols = x_ref.shape
    wide = w_ref.shape[1]
    heads = cols // SSD_HEAD
    groups = wide // STATE
    per = heads // groups
    margin = CONV // 2
    start = 0
    for src, taps, dst in ((x_ref, tx_ref, xs), (w_ref, tw_ref, ws), (r_ref, tr_ref, read_ref)):
        span = src.shape[1]
        line[0:EDGE, 0:span] = prev_ref[:, start : start + span].astype(F32)
        line[EDGE : EDGE + rows, 0:span] = src[...].astype(F32)
        line[EDGE + rows : 2 * EDGE + rows, 0:span] = next_ref[:, start : start + span].astype(F32)
        step = min(span, 256)
        for at in range(0, span, step):
            total = jnp.zeros((rows, step), F32)
            for k in range(CONV):
                low = EDGE - margin + k
                total = total + line[low : low + rows, at : at + step] * taps[
                    k : k + 1, at : at + step
                ].astype(F32)
            dst[:, at : at + step] = silu(total).astype(BF16)
        start += span

    steps = jax.nn.softplus(inc_ref[...])
    logs = -jnp.exp(fade_ref[...]) * steps + spike_ref[...]
    first = lax.broadcasted_iota(jnp.int32, (rows, rows), 0)
    second = lax.broadcasted_iota(jnp.int32, (rows, rows), 1)
    lower = first >= second
    upper = first <= second
    run_f = nn(logs[0:heads], jnp.where(upper, 1.0, 0.0), HIGHEST)
    run_b = nn(logs[heads : 2 * heads], jnp.where(lower, 1.0, 0.0), HIGHEST)
    tall = jnp.concatenate([run_f, run_b], axis=0).T
    expl_ref[...] = jnp.exp(tall)
    tot_f = run_f[:, rows - 1 : rows]
    tot_b = run_b[:, 0:1]
    end_f = jnp.exp(tot_f - run_f) * steps[0:heads]
    end_b = jnp.exp(tot_b - run_b) * steps[heads : 2 * heads]

    spread = head_spread(heads, cols)
    tot = jnp.exp(jnp.concatenate([tall[rows - 1 : rows, 0:heads], tall[0:1, heads:]], axis=0))
    tot = nn(tot, spread, HIGHEST)
    high = tot.astype(BF16)
    low = (tot - high.astype(F32)).astype(BF16)
    half = cols // 2
    tail = jnp.concatenate(
        [high.astype(F32), low.astype(F32), jnp.zeros((EDGE - 4, cols), F32)], axis=0
    ).astype(BF16)
    for side in range(2):
        part = tail[:, side * half : (side + 1) * half]

        @pl.when(place[0] == side)
        def _():
            keep_ref[2 * STATE : 2 * STATE + EDGE, :] = part

        @pl.when(place[0] != side)
        def _():
            send_ref[2 * STATE : 2 * STATE + EDGE, :] = part

    for g in range(groups):
        wg = ws[:, g * STATE : (g + 1) * STATE]
        rg = read_ref[:, g * STATE : (g + 1) * STATE]
        affinity = nt(rg, wg)
        turned = wg.astype(F32).T
        fresh = []
        for j in range(per):
            h = g * per + j
            at = h * SSD_HEAD
            ahead = jnp.exp(
                jnp.where(lower, tall[:, h : h + 1] - run_f[h : h + 1, :], -jnp.inf)
            ) * steps[h : h + 1, :]
            back = jnp.exp(
                jnp.where(
                    upper, tall[:, heads + h : heads + h + 1] - run_b[h : h + 1, :], -jnp.inf
                )
            ) * steps[heads + h : heads + h + 1, :]
            mixed = (affinity * (ahead + back)).astype(BF16)
            grow_f = (turned * end_f[h : h + 1, :]).astype(BF16)
            grow_b = (turned * end_b[h : h + 1, :]).astype(BF16)
            got = nn(jnp.concatenate([mixed, grow_f, grow_b], axis=0), xs[:, at : at + SSD_HEAD])
            y_ref[:, at : at + SSD_HEAD] = got[0:rows]
            fresh.append(got[rows : rows + 2 * STATE].astype(BF16))
        whole = jnp.concatenate(fresh, axis=1)
        size = per * SSD_HEAD
        base = g * size
        for side in range(2):
            a = max(base, side * half)
            b = min(base + size, (side + 1) * half)
            if a >= b:
                continue
            part = whole[:, a - base : b - base]

            @pl.when(place[0] == side)
            def _():
                keep_ref[0 : 2 * STATE, a - side * half : b - side * half] = part

            @pl.when(place[0] != side)
            def _():
                send_ref[0 : 2 * STATE, a - side * half : b - side * half] = part


def attend_kernel(
    place, sink, q_ref, k_ref, v_ref, prev_ref, next_ref, cos_ref, sin_ref, out_ref
):
    rows = q_ref.shape[0]
    kv = k_ref.shape[1] // HEAD
    sharing = q_ref.shape[1] // k_ref.shape[1]
    wide = k_ref.shape[1]

    def turn(m, low):
        m = m.astype(F32)
        half = HEAD // 2
        other = jnp.concatenate([m[:, half:], m[:, :half]], axis=1)
        high = low + m.shape[0]
        return (m * cos_ref[low:high, :] + other * sin_ref[low:high, :]).astype(BF16)

    within = lax.broadcasted_iota(jnp.int32, (rows, 3 * rows), 0)
    across = lax.broadcasted_iota(jnp.int32, (rows, 3 * rows), 1)
    far = across - rows - within
    allowed = (far <= WINDOW) & (far >= -WINDOW)
    allowed = allowed & ((across >= rows) | (place[0] > 0))
    allowed = allowed & ((across < 2 * rows) | (place[0] < place[1] - 1))
    for g in range(kv):
        at = g * HEAD
        keys = jnp.concatenate(
            [
                turn(prev_ref[:, at : at + HEAD], 0),
                turn(k_ref[:, at : at + HEAD], rows),
                turn(next_ref[:, at : at + HEAD], 2 * rows),
            ],
            axis=0,
        )
        values = jnp.concatenate(
            [
                prev_ref[:, wide + at : wide + at + HEAD],
                v_ref[:, at : at + HEAD],
                next_ref[:, wide + at : wide + at + HEAD],
            ],
            axis=0,
        )
        for j in range(sharing):
            h = g * sharing + j
            query = turn(q_ref[:, h * HEAD : (h + 1) * HEAD], rows)
            scores = nt(query, keys) * HEAD ** (-0.5)
            scores = jnp.where(allowed, scores, -jnp.inf)
            top = jnp.maximum(jnp.max(scores, axis=1, keepdims=True), sink[h])
            weights = jnp.exp(scores - top)
            total = jnp.sum(weights, axis=1, keepdims=True) + jnp.exp(sink[h] - top)
            chance = (weights / total).astype(BF16)
            out_ref[:, h * HEAD : (h + 1) * HEAD] = nn(chance, values).astype(BF16)


def finish_kernel(place, y_ref, read_ref, expl_ref, own_ref, got_ref, gate_ref, gain_ref, out_ref):
    _, cols = y_ref.shape
    wide = read_ref.shape[1]
    heads = cols // SSD_HEAD
    groups = wide // STATE
    size = cols // groups
    half = cols // 2
    spread = head_spread(heads, cols)
    for g in range(groups):
        at = g * size
        rg = read_ref[:, g * STATE : (g + 1) * STATE]
        pieces = []
        for low in range(at, at + size, min(size, half)):
            span = min(size, half)
            side = low // half
            off = low - side * half
            mine = place[0] == side
            pieces.append(
                jnp.where(
                    mine,
                    own_ref[:, off : off + span].astype(F32),
                    got_ref[:, off : off + span].astype(F32),
                ).astype(BF16)
            )
        states = pieces[0] if len(pieces) == 1 else jnp.concatenate(pieces, axis=1)
        local = spread[:, at : at + size]
        fade_f = nn(expl_ref[:, 0:heads], local, HIGHEST)
        fade_b = nn(expl_ref[:, heads : 2 * heads], local, HIGHEST)
        both = (
            y_ref[:, at : at + size]
            + fade_f * nn(rg, states[0:STATE])
            + fade_b * nn(rg, states[STATE : 2 * STATE])
        )
        gated = both * silu(gate_ref[:, at : at + size].astype(F32))
        mean = jnp.sum(gated * gated, axis=1, keepdims=True) * (1.0 / size)
        out_ref[:, at : at + size] = (
            gated * lax.rsqrt(mean + EPSILON) * gain_ref[:, at : at + size]
        ).astype(BF16)


def first_kernel(count, *refs):
    lefts = refs[: count[0]]
    shards = refs[count[0] : count[0] + count[1]]
    out_ref = refs[-1]
    left = jnp.concatenate([a[...] for a in lefts], axis=0)
    at = 0
    for shard in shards:
        span = shard.shape[1]
        out_ref[:, at : at + span] = nn(left, shard[...])
        at += span


def second_kernel(count, place, sum_ref, *refs):
    lefts = refs[: count[0]]
    shards = refs[count[0] : count[0] + count[1]]
    outs = refs[count[0] + count[1] :]
    rows = lefts[0].shape[0]
    half = rows // 2
    left = jnp.concatenate([a[...] for a in lefts], axis=0)
    at = 0
    for shard in shards:
        span = shard.shape[1]
        total = (sum_ref[:, at : at + span] + nn(left, shard[...])).astype(BF16)
        for side in range(2):

            @pl.when(place[0] == side)
            def _():
                for i in range(count[0]):
                    a = i * rows + side * half
                    b = i * rows + (1 - side) * half
                    outs[2 * i][:, at : at + span] = total[a : a + half]
                    outs[2 * i + 1][:, at : at + span] = total[b : b + half]

        at += span


def place_kernel(shape, place, *refs):
    sources, columns, span = shape
    out_ref = refs[-1]
    for i in range(sources):
        for j in range(columns):
            at = j * span
            to = pl.multiple_of(place[i * columns + j] * span, span)
            out_ref[:, pl.ds(to, span)] = (
                refs[2 * i][:, at : at + span].astype(F32)
                + refs[2 * i + 1][:, at : at + span].astype(F32)
            ).astype(BF16)


def flip(a, count, mask):
    return lax.ppermute(a, "sp", [(i, i ^ mask) for i in range(count)])


def shift(a, count, by):
    return lax.ppermute(
        a, "sp", [(i, i + by) for i in range(count) if 0 <= i + by < count]
    )


def cross(a, count, mask):
    return lax.ppermute(
        a,
        ("sp", "tp"),
        [(2 * i + j, 2 * (i ^ mask) + 1 - j) for i in range(count) for j in range(2)],
    )


def exchange_states(keep, send, count, me):
    half = keep.shape[1]
    core = me & 1
    got = flip(send, count, 1)

    def split(a):
        tail = a[2 * STATE :].astype(F32)
        return (
            a[:STATE].astype(F32),
            a[STATE : 2 * STATE].astype(F32),
            tail[0:1] + tail[2:3],
            tail[1:2] + tail[3:4],
        )

    mine = split(keep)
    theirs = split(got)
    pick = lambda flag, a, b: jax.tree.map(lambda u, v: jnp.where(flag, u, v), a, b)
    low = pick(core == 0, mine, theirs)
    high = pick(core == 0, theirs, mine)
    join = lambda low, high: (
        low[0] * high[2] + high[0],
        high[1] * low[3] + low[1],
        low[2] * high[2],
        low[3] * high[3],
    )
    pair = (low, high)
    total = join(low, high)
    into_f = jnp.zeros((STATE, half), F32)
    into_b = jnp.zeros((STATE, half), F32)
    gap_f = jnp.ones((1, half), F32)
    gap_b = jnp.ones((1, half), F32)
    bit = 2
    while bit < count:
        upper = (me & bit) != 0
        last = bit * 2 >= count
        if last:
            payload = jnp.where(upper, total[1], total[0]).astype(BF16)
            other = flip(payload, count, bit).astype(F32)
            into_f = jnp.where(upper, other * gap_f + into_f, into_f)
            into_b = jnp.where(upper, into_b, other * gap_b + into_b)
        else:
            fades = jnp.concatenate([total[2], total[3]], axis=0)
            top = fades.astype(BF16)
            rest = (fades - top.astype(F32)).astype(BF16)
            payload = jnp.concatenate(
                [
                    total[0].astype(BF16),
                    total[1].astype(BF16),
                    top,
                    rest,
                    jnp.zeros((EDGE - 4, half), BF16),
                ],
                axis=0,
            )
            other = split(flip(payload, count, bit))
            low = pick(upper, other, total)
            high = pick(upper, total, other)
            into_f = jnp.where(upper, other[0] * gap_f + into_f, into_f)
            into_b = jnp.where(upper, into_b, other[1] * gap_b + into_b)
            gap_f = jnp.where(upper, gap_f * other[2], gap_f)
            gap_b = jnp.where(upper, gap_b, gap_b * other[3])
            total = join(low, high)
        bit *= 2
    low, high = pair
    first = jnp.concatenate([into_f, into_b * high[3] + high[1]], axis=0).astype(BF16)
    second = jnp.concatenate([into_f * low[2] + low[0], into_b], axis=0).astype(BF16)
    own = jnp.where(core == 0, first, second)
    away = jnp.where(core == 0, second, first)
    return own, flip(away, count, 1)


def local(
    asking_matrix,
    matching_key_matrix,
    carried_value_matrix,
    silu_switch_argument,
    duality_source_matrix,
    storing_direction_matrix,
    fetching_direction_matrix,
    duality_kernel_coefficients,
    storing_kernel_coefficients,
    fetching_kernel_coefficients,
    raw_increment_lengths,
    logarithmic_fading_speeds,
    token_fading_spikes,
    absorber_score_vector,
    cluster_scaling_factor,
    final_mapping_matrix,
):
    rows = asking_matrix.shape[0]
    me = lax.axis_index("sp")
    side = lax.axis_index("tp")
    count = lax.axis_size("sp")
    tps = lax.axis_size("tp")
    cols = duality_source_matrix.shape[1]
    wide = storing_direction_matrix.shape[1]
    heads = cols // SSD_HEAD
    core = (me & 1).astype(jnp.int32).reshape(1)
    sds = jax.ShapeDtypeStruct

    raw = (duality_source_matrix, storing_direction_matrix, fetching_direction_matrix)
    tail = jnp.concatenate([a[rows - EDGE :] for a in raw], axis=1)
    lead = jnp.concatenate([a[:EDGE] for a in raw], axis=1)
    prev_edge = shift(tail, count, 1)
    next_edge = shift(lead, count, -1)
    pairs = jnp.concatenate([matching_key_matrix, carried_value_matrix], axis=1)
    prev_pair = shift(pairs, count, 1)
    next_pair = shift(pairs, count, -1)

    span = final_mapping_matrix.shape[2]
    fast = tps == 2 and span % 128 == 0 and count == 16
    shared = [1, 4] if fast else [1]
    bits = []
    bit = count // 2
    while bit >= 2:
        if bit not in shared:
            bits.append(bit)
        bit //= 2
    halves = [{0: final_mapping_matrix[0]}, {0: final_mapping_matrix[1]}]
    for shards in halves:
        for bit in bits:
            for mask in list(shards):
                shards[mask ^ bit] = flip(shards[mask], count, bit)
    masks = list(halves[0])

    keep, send, read, inner, expl = call(
        block_kernel,
        [
            sds((2 * STATE + EDGE, cols // 2), BF16),
            sds((2 * STATE + EDGE, cols // 2), BF16),
            sds((rows, wide), BF16),
            sds((rows, cols), F32),
            sds((rows, 2 * heads), F32),
        ],
        [
            core,
            *raw,
            prev_edge,
            next_edge,
            duality_kernel_coefficients,
            storing_kernel_coefficients,
            fetching_kernel_coefficients,
            raw_increment_lengths.reshape(2 * heads, rows),
            logarithmic_fading_speeds.reshape(2 * heads, 1),
            token_fading_spikes.reshape(2 * heads, rows),
        ],
        flops=4 * 10**9,
        scratch=[
            pltpu.VMEM((rows + 2 * EDGE, max(cols, wide)), F32),
            pltpu.VMEM((rows, cols), BF16),
            pltpu.VMEM((rows, wide), BF16),
        ],
    )
    own_state, got_state = exchange_states(keep, send, count, me)

    halfway = HEAD // 2
    spacing = ROTARY_BASE ** (-jnp.arange(halfway, dtype=F32) * 2.0 / HEAD)
    places = ((me - 1) * rows + jnp.arange(3 * rows, dtype=jnp.int32)).astype(F32)
    angles = places[:, None] * spacing[None, :]
    cosine = jnp.cos(angles)
    sine = jnp.sin(angles)
    cosine = jnp.concatenate([cosine, cosine], axis=1)
    sine = jnp.concatenate([-sine, sine], axis=1)
    where = jnp.stack([me, jnp.int32(count)]).astype(jnp.int32)
    (attended,) = call(
        attend_kernel,
        [sds(asking_matrix.shape, BF16)],
        [
            where,
            absorber_score_vector,
            asking_matrix,
            matching_key_matrix,
            carried_value_matrix,
            prev_pair,
            next_pair,
            cosine,
            sine,
        ],
        flops=3 * 10**9,
        scalars=2,
    )

    def spread_rows(a):
        blocks = [a]
        for bit in reversed(shared):
            blocks += [flip(b, count, bit) for b in blocks]
        return blocks

    attended_blocks = spread_rows(attended)

    (normed,) = call(
        finish_kernel,
        [sds((rows, cols), BF16)],
        [
            core,
            inner,
            read,
            expl,
            own_state,
            got_state,
            silu_switch_argument,
            cluster_scaling_factor.reshape(1, cols),
        ],
        flops=3 * 10**9,
    )
    normed_blocks = spread_rows(normed)
    if fast:
        group = [0, 4, 1, 5]
        width = span * len(masks)
        sizes = (len(group), len(masks))
        flops = 2 * len(group) * rows * cols * width
        (early,) = call(
            functools.partial(first_kernel, sizes),
            [sds((len(group) * rows, width), F32)],
            [*attended_blocks, *[halves[0][m] for m in masks]],
            flops=flops,
            scalars=0,
        )
        outs = call(
            functools.partial(second_kernel, sizes),
            [sds((rows // 2, width), BF16)] * (2 * len(group)),
            [
                side.astype(jnp.int32).reshape(1),
                early,
                *normed_blocks,
                *[halves[1][m] for m in masks],
            ],
            flops=flops,
        )
        pieces = []
        order = []
        for i, m in enumerate(group):
            pieces.append(outs[2 * i] if m == 0 else flip(outs[2 * i], count, m))
            pieces.append(cross(outs[2 * i + 1], count, m))
            order += [me ^ m ^ b for b in masks]
        (out,) = call(
            functools.partial(place_kernel, (len(group), len(masks), span)),
            [sds((rows // 2, span * count), BF16)],
            [jnp.stack(order).astype(jnp.int32), *pieces],
            flops=10**6,
        )
        return out

    attended_pair = attended_blocks[1]
    normed_pair = normed_blocks[1]
    shards = {m: jnp.stack([halves[0][m], halves[1][m]]) for m in masks}
    left = jnp.concatenate(
        [
            jnp.concatenate([attended, normed], axis=1),
            jnp.concatenate([attended_pair, normed_pair], axis=1),
        ],
        axis=0,
    )
    stacked = jnp.concatenate([shards[m] for m in masks], axis=2).reshape(
        -1, span * len(masks)
    )
    partial = jnp.dot(left, stacked, preferred_element_type=F32).astype(BF16)
    partial = partial.reshape(2, tps, rows // tps, -1)
    summed = lax.psum_scatter(partial, "tp", scatter_dimension=1, tiled=True)
    summed = summed.reshape(2, rows // tps, len(masks), span)
    own, away = summed[0], flip(summed[1], count, 1)
    full = [None] * count
    for j, m in enumerate(masks):
        full[m] = own[:, j]
        full[m ^ 1] = away[:, j]
    full = jnp.stack(full, axis=0)
    bit = 1
    while bit < count:
        seen = full.reshape(count // (2 * bit), 2, bit, rows // tps, span)
        full = jnp.where((me & bit) != 0, seen[:, ::-1], seen).reshape(full.shape)
        bit *= 2
    return jnp.moveaxis(full, 0, 1).reshape(rows // tps, count * span)


def solution(mesh):
    in_specs = (
        P("sp", "tp"),
        P("sp", "tp"),
        P("sp", "tp"),
        P("sp", "tp"),
        P("sp", "tp"),
        P("sp", "tp"),
        P("sp", "tp"),
        P(None, "tp"),
        P(None, "tp"),
        P(None, "tp"),
        P(None, "tp", "sp"),
        P(None, "tp"),
        P(None, "tp", "sp"),
        P("tp"),
        P("tp"),
        P(None, "tp", "sp"),
    )
    out_specs = P(("sp", "tp"), None)

    return jax.shard_map(local, mesh=mesh, in_specs=in_specs, out_specs=out_specs, check_vma=False)
```

```python
import functools

import jax
import jax.numpy as jnp
from jax import lax
from jax.experimental import pallas as pl
from jax.experimental.pallas import tpu as pltpu
from jax.sharding import PartitionSpec as P


HEAD = 128
SSD_HEAD = 64
STATE = 128
CONV = 5
WINDOW = 128
EDGE = 16

ROTARY_BASE = 500000.0
EPSILON = 1e-06
HIGHEST = lax.Precision.HIGHEST
F32 = jnp.float32
BF16 = jnp.bfloat16
VMEM = pl.BlockSpec(memory_space=pltpu.VMEM)
SMEM = pl.BlockSpec(memory_space=pltpu.SMEM)


def call(kernel, outs, ins, flops, scratch=(), scalars=0):
    moved = sum(a.size * a.dtype.itemsize for a in list(ins) + list(outs))
    return pl.pallas_call(
        kernel,
        out_shape=outs,
        in_specs=[SMEM] * scalars + [VMEM] * (len(ins) - scalars),
        out_specs=[VMEM] * len(outs),
        scratch_shapes=list(scratch),
        cost_estimate=pl.CostEstimate(flops=flops, bytes_accessed=moved, transcendentals=0),
    )(*ins)


def nn(a, b, precision=None):
    return lax.dot_general(
        a, b, (((1,), (0,)), ((), ())), precision=precision, preferred_element_type=F32
    )


def nt(a, b, precision=None):
    return lax.dot_general(
        a, b, (((1,), (1,)), ((), ())), precision=precision, preferred_element_type=F32
    )


def silu(v):
    return v / (1.0 + jnp.exp(-v))


def head_spread(heads, cols):
    head = lax.broadcasted_iota(jnp.int32, (heads, cols), 0)
    col = lax.broadcasted_iota(jnp.int32, (heads, cols), 1)
    return jnp.where(col // SSD_HEAD == head, 1.0, 0.0).astype(F32)


def block_kernel(
    x_ref,
    w_ref,
    r_ref,
    pair_ref,
    outer_ref,
    tx_ref,
    tw_ref,
    tr_ref,
    inc_ref,
    fade_ref,
    spike_ref,
    keep_ref,
    send_ref,
    read_ref,
    y_ref,
    expl_ref,
    line,
    xs,
    ws,
):
    rows, cols = x_ref.shape
    wide = w_ref.shape[1]
    core = lax.axis_index("sp") & 1
    heads = cols // SSD_HEAD
    groups = wide // STATE
    per = heads // groups
    margin = CONV // 2
    start = 0
    for src, taps, dst in ((x_ref, tx_ref, xs), (w_ref, tw_ref, ws), (r_ref, tr_ref, read_ref)):
        span = src.shape[1]
        pair = pair_ref[:, start : start + span].astype(F32)
        outer = outer_ref[:, start : start + span].astype(F32)
        line[0:EDGE, 0:span] = jnp.where(core == 0, outer, pair)
        line[EDGE : EDGE + rows, 0:span] = src[...].astype(F32)
        line[EDGE + rows : 2 * EDGE + rows, 0:span] = jnp.where(core == 0, pair, outer)
        step = min(span, 256)
        for at in range(0, span, step):
            total = jnp.zeros((rows, step), F32)
            for k in range(CONV):
                low = EDGE - margin + k
                total = total + line[low : low + rows, at : at + step] * taps[
                    k : k + 1, at : at + step
                ].astype(F32)
            dst[:, at : at + step] = silu(total).astype(BF16)
        start += span

    steps = jax.nn.softplus(inc_ref[...])
    square = lax.broadcasted_iota(jnp.int32, (heads, heads), 0)
    square = square == lax.broadcasted_iota(jnp.int32, (heads, heads), 1)
    rates = jnp.concatenate(
        [
            jnp.sum(jnp.where(square, jnp.exp(fade_ref[d : d + 1, :]), 0.0), axis=1, keepdims=True)
            for d in range(2)
        ],
        axis=0,
    )
    logs = -rates * steps + spike_ref[...]
    first = lax.broadcasted_iota(jnp.int32, (rows, rows), 0)
    second = lax.broadcasted_iota(jnp.int32, (rows, rows), 1)
    lower = first >= second
    upper = first <= second
    run_f = nn(logs[0:heads], jnp.where(upper, 1.0, 0.0), HIGHEST)
    run_b = nn(logs[heads : 2 * heads], jnp.where(lower, 1.0, 0.0), HIGHEST)
    tall = jnp.concatenate([run_f, run_b], axis=0).T
    expl_ref[...] = jnp.exp(tall)
    tot_f = run_f[:, rows - 1 : rows]
    tot_b = run_b[:, 0:1]
    end_f = jnp.exp(tot_f - run_f) * steps[0:heads]
    end_b = jnp.exp(tot_b - run_b) * steps[heads : 2 * heads]

    spread = head_spread(heads, cols)
    tot = jnp.exp(jnp.concatenate([tall[rows - 1 : rows, 0:heads], tall[0:1, heads:]], axis=0))
    tot = nn(tot, spread, HIGHEST)
    high = tot.astype(BF16)
    low = (tot - high.astype(F32)).astype(BF16)
    half = cols // 2
    tail = jnp.concatenate(
        [high.astype(F32), low.astype(F32), jnp.zeros((EDGE - 4, cols), F32)], axis=0
    ).astype(BF16)
    for side in range(2):
        part = tail[:, side * half : (side + 1) * half]

        @pl.when(core == side)
        def _():
            keep_ref[2 * STATE : 2 * STATE + EDGE, :] = part

        @pl.when(core != side)
        def _():
            send_ref[2 * STATE : 2 * STATE + EDGE, :] = part

    for g in range(groups):
        wg = ws[:, g * STATE : (g + 1) * STATE]
        rg = read_ref[:, g * STATE : (g + 1) * STATE]
        affinity = nt(rg, wg)
        turned = wg.astype(F32).T
        fresh = []
        for j in range(per):
            h = g * per + j
            at = h * SSD_HEAD
            ahead = jnp.exp(
                jnp.where(lower, tall[:, h : h + 1] - run_f[h : h + 1, :], -jnp.inf)
            ) * steps[h : h + 1, :]
            back = jnp.exp(
                jnp.where(
                    upper, tall[:, heads + h : heads + h + 1] - run_b[h : h + 1, :], -jnp.inf
                )
            ) * steps[heads + h : heads + h + 1, :]
            mixed = (affinity * (ahead + back)).astype(BF16)
            grow_f = (turned * end_f[h : h + 1, :]).astype(BF16)
            grow_b = (turned * end_b[h : h + 1, :]).astype(BF16)
            got = nn(jnp.concatenate([mixed, grow_f, grow_b], axis=0), xs[:, at : at + SSD_HEAD])
            y_ref[:, at : at + SSD_HEAD] = got[0:rows]
            fresh.append(got[rows : rows + 2 * STATE].astype(BF16))
        whole = jnp.concatenate(fresh, axis=1)
        size = per * SSD_HEAD
        base = g * size
        for side in range(2):
            a = max(base, side * half)
            b = min(base + size, (side + 1) * half)
            if a >= b:
                continue
            part = whole[:, a - base : b - base]

            @pl.when(core == side)
            def _():
                keep_ref[0 : 2 * STATE, a - side * half : b - side * half] = part

            @pl.when(core != side)
            def _():
                send_ref[0 : 2 * STATE, a - side * half : b - side * half] = part


def attend_kernel(
    sink, q_ref, k_ref, v_ref, pair_ref, outer_ref, cos_ref, sin_ref, out_ref
):
    rows = q_ref.shape[0]
    me = lax.axis_index("sp")
    last = lax.axis_size("sp") - 1
    kv = k_ref.shape[1] // HEAD
    sharing = q_ref.shape[1] // k_ref.shape[1]
    wide = k_ref.shape[1]

    def turn(m, low):
        m = m.astype(F32)
        half = HEAD // 2
        other = jnp.concatenate([m[:, half:], m[:, :half]], axis=1)
        high = low + m.shape[0]
        return (m * cos_ref[low:high, :] + other * sin_ref[low:high, :]).astype(BF16)

    within = lax.broadcasted_iota(jnp.int32, (rows, 3 * rows), 0)
    across = lax.broadcasted_iota(jnp.int32, (rows, 3 * rows), 1)
    far = across - rows - within
    allowed = (far <= WINDOW) & (far >= -WINDOW)
    allowed = allowed & ((across >= rows) | (me > 0))
    allowed = allowed & ((across < 2 * rows) | (me < last))
    even = (me & 1) == 0
    for g in range(kv):
        at = g * HEAD
        near = [
            (pair_ref[:, a : a + HEAD].astype(F32), outer_ref[:, a : a + HEAD].astype(F32))
            for a in (at, wide + at)
        ]
        before = [jnp.where(even, o, p) for p, o in near]
        after = [jnp.where(even, p, o) for p, o in near]
        keys = jnp.concatenate(
            [
                turn(before[0], 0),
                turn(k_ref[:, at : at + HEAD], rows),
                turn(after[0], 2 * rows),
            ],
            axis=0,
        )
        values = jnp.concatenate(
            [
                before[1].astype(BF16),
                v_ref[:, at : at + HEAD],
                after[1].astype(BF16),
            ],
            axis=0,
        )
        for j in range(sharing):
            h = g * sharing + j
            query = turn(q_ref[:, h * HEAD : (h + 1) * HEAD], rows)
            scores = nt(query, keys) * HEAD ** (-0.5)
            scores = jnp.where(allowed, scores, -jnp.inf)
            top = jnp.maximum(jnp.max(scores, axis=1, keepdims=True), sink[h])
            weights = jnp.exp(scores - top)
            total = jnp.sum(weights, axis=1, keepdims=True) + jnp.exp(sink[h] - top)
            chance = (weights / total).astype(BF16)
            out_ref[:, h * HEAD : (h + 1) * HEAD] = nn(chance, values).astype(BF16)


def finish_kernel(y_ref, read_ref, expl_ref, own_ref, got_ref, gate_ref, gain_ref, out_ref):
    _, cols = y_ref.shape
    core = lax.axis_index("sp") & 1
    wide = read_ref.shape[1]
    heads = cols // SSD_HEAD
    groups = wide // STATE
    size = cols // groups
    half = cols // 2
    spread = head_spread(heads, cols)
    for g in range(groups):
        at = g * size
        rg = read_ref[:, g * STATE : (g + 1) * STATE]
        pieces = []
        for low in range(at, at + size, min(size, half)):
            span = min(size, half)
            side = low // half
            off = low - side * half
            mine = core == side
            pieces.append(
                jnp.where(
                    mine,
                    own_ref[:, off : off + span].astype(F32),
                    got_ref[:, off : off + span].astype(F32),
                ).astype(BF16)
            )
        states = pieces[0] if len(pieces) == 1 else jnp.concatenate(pieces, axis=1)
        local = spread[:, at : at + size]
        fade_f = nn(expl_ref[:, 0:heads], local, HIGHEST)
        fade_b = nn(expl_ref[:, heads : 2 * heads], local, HIGHEST)
        both = (
            y_ref[:, at : at + size]
            + fade_f * nn(rg, states[0:STATE])
            + fade_b * nn(rg, states[STATE : 2 * STATE])
        )
        gated = both * silu(gate_ref[:, at : at + size].astype(F32))
        mean = jnp.sum(gated * gated, axis=1, keepdims=True) * (1.0 / size)
        out_ref[:, at : at + size] = (
            gated * lax.rsqrt(mean + EPSILON) * gain_ref[:, at : at + size]
        ).astype(BF16)


def first_kernel(count, *refs):
    lefts = refs[: count[0]]
    shards = refs[count[0] : count[0] + count[1]]
    out_ref = refs[-1]
    left = jnp.concatenate([a[...] for a in lefts], axis=0)
    at = 0
    for shard in shards:
        span = shard.shape[1]
        out_ref[:, at : at + span] = nn(left, shard[...])
        at += span


def second_kernel(count, sum_ref, *refs):
    place = lax.axis_index("tp")
    blocks, shards, base = count
    lefts = refs[:blocks]
    tops = refs[blocks : blocks + shards]
    lows = refs[blocks + shards : blocks + 2 * shards]
    outs = refs[blocks + 2 * shards :]
    rows = lefts[0].shape[0]
    half = rows // 2
    deep = tops[0].shape[0]
    left = jnp.concatenate([a[...] for a in lefts], axis=0)
    at = 0
    for top, low in zip(tops, lows):
        span = top.shape[1]
        total = (
            sum_ref[:, base + at : base + at + span]
            + nn(left[:, :deep], top[...])
            + nn(left[:, deep:], low[...])
        ).astype(BF16)
        for side in range(2):

            @pl.when(place == side)
            def _():
                for i in range(blocks):
                    a = i * rows + side * half
                    b = i * rows + (1 - side) * half
                    outs[2 * i][:, at : at + span] = total[a : a + half]
                    outs[2 * i + 1][:, at : at + span] = total[b : b + half]

        at += span


def place_kernel(group, masks, span, *refs):
    me = lax.axis_index("sp")
    out_ref = refs[-1]
    for i, block in enumerate(group):
        for j, mask in enumerate(masks):
            at = j * span
            to = pl.multiple_of((me ^ (block ^ mask)) * span, span)
            out_ref[:, pl.ds(to, span)] = (
                refs[2 * i][:, at : at + span].astype(F32)
                + refs[2 * i + 1][:, at : at + span].astype(F32)
            ).astype(BF16)


def edge_kernel(*refs):
    even = (lax.axis_index("sp") & 1) == 0
    start = 0
    for i in range(0, 6, 2):
        lead = refs[i][...].astype(F32)
        tail = refs[i + 1][...].astype(F32)
        span = lead.shape[1]
        refs[6][:, start : start + span] = jnp.where(even, tail, lead).astype(BF16)
        refs[7][:, start : start + span] = jnp.where(even, lead, tail).astype(BF16)
        start += span


def edges(raw):
    specs = []
    for a in raw:
        end = a.shape[0] // EDGE - 1
        specs.append(pl.BlockSpec((EDGE, a.shape[1]), lambda i: (0, 0)))
        specs.append(pl.BlockSpec((EDGE, a.shape[1]), lambda i, end=end: (end, 0)))
    width = sum(a.shape[1] for a in raw)
    return pl.pallas_call(
        edge_kernel,
        grid=(1,),
        out_shape=[jax.ShapeDtypeStruct((EDGE, width), BF16)] * 2,
        in_specs=specs,
        out_specs=[pl.BlockSpec((EDGE, width), lambda i: (0, 0))] * 2,
        name="edges",
    )(*[a for a in raw for _ in range(2)])


def join_kernel(keep_ref, got_ref, out_ref):
    even = (lax.axis_index("sp") & 1) == 0
    end = 2 * STATE

    def load(low, high):
        mine = keep_ref[low:high, :].astype(F32)
        theirs = got_ref[low:high, :].astype(F32)
        return jnp.where(even, mine, theirs), jnp.where(even, theirs, mine)

    low, high = load(end, end + EDGE)
    low = low[0:2] + low[2:4]
    high = high[0:2] + high[2:4]
    fades = low * high
    top = fades.astype(BF16).astype(F32)
    rest = fades - top
    out_ref[end : end + EDGE, :] = jnp.concatenate(
        [top, rest, jnp.zeros((EDGE - 4, top.shape[1]), F32)], axis=0
    ).astype(BF16)
    a, b = load(0, STATE)
    out_ref[0:STATE, :] = (a * high[0:1] + b).astype(BF16)
    a, b = load(STATE, end)
    out_ref[STATE:end, :] = (b * low[1:2] + a).astype(BF16)


def flip(a, count, mask):
    return lax.ppermute(a, "sp", [(i, i ^ mask) for i in range(count)])


def outer(a, count):
    pairs = [(i, i + 1) for i in range(1, count - 1, 2)]
    return lax.ppermute(a, "sp", pairs + [(j, i) for i, j in pairs])


def cross(a, count, mask):
    return lax.ppermute(
        a,
        ("sp", "tp"),
        [(2 * i + j, 2 * (i ^ mask) + 1 - j) for i in range(count) for j in range(2)],
    )


def join_pair(keep, got):
    (payload,) = call(
        join_kernel, [jax.ShapeDtypeStruct(keep.shape, BF16)], [keep, got], flops=10**6
    )
    return payload


def exchange_states(keep, send, count, me):
    half = keep.shape[1]
    core = me & 1
    got = flip(send, count, 1)

    def split(a):
        tail = a[2 * STATE :].astype(F32)
        return (
            a[:STATE].astype(F32),
            a[STATE : 2 * STATE].astype(F32),
            tail[0:1] + tail[2:3],
            tail[1:2] + tail[3:4],
        )

    pick = lambda flag, a, b: jax.tree.map(lambda u, v: jnp.where(flag, u, v), a, b)
    join = lambda low, high: (
        low[0] * high[2] + high[0],
        high[1] * low[3] + low[1],
        low[2] * high[2],
        low[3] * high[3],
    )

    def pack(total):
        fades = jnp.concatenate([total[2], total[3]], axis=0)
        top = fades.astype(BF16)
        rest = (fades - top.astype(F32)).astype(BF16)
        return jnp.concatenate(
            [
                total[0].astype(BF16),
                total[1].astype(BF16),
                top,
                rest,
                jnp.zeros((EDGE - 4, half), BF16),
            ],
            axis=0,
        )

    seen = payload = join_pair(keep, got)
    total = split(payload)
    into_f = jnp.zeros((STATE, half), F32)
    into_b = jnp.zeros((STATE, half), F32)
    gap_f = jnp.ones((1, half), F32)
    gap_b = jnp.ones((1, half), F32)
    bit = 2
    while bit < count:
        upper = (me & bit) != 0
        last = bit * 2 >= count
        if last:
            payload = jnp.where(upper, total[1], total[0]).astype(BF16)
            other = flip(payload, count, bit).astype(F32)
            into_f = jnp.where(upper, other * gap_f + into_f, into_f)
            into_b = jnp.where(upper, into_b, other * gap_b + into_b)
        else:
            if payload is None:
                payload = pack(total)
            other = split(flip(payload, count, bit))
            payload = None
            low = pick(upper, other, total)
            high = pick(upper, total, other)
            into_f = jnp.where(upper, other[0] * gap_f + into_f, into_f)
            into_b = jnp.where(upper, into_b, other[1] * gap_b + into_b)
            gap_f = jnp.where(upper, gap_f * other[2], gap_f)
            gap_b = jnp.where(upper, gap_b, gap_b * other[3])
            total = join(low, high)
        bit *= 2
    keep, got = lax.optimization_barrier((keep, got, seen))[:2]
    mine, theirs = split(keep), split(got)
    low = pick(core == 0, mine, theirs)
    high = pick(core == 0, theirs, mine)
    first = jnp.concatenate([into_f, into_b * high[3] + high[1]], axis=0).astype(BF16)
    second = jnp.concatenate([into_f * low[2] + low[0], into_b], axis=0).astype(BF16)
    own = jnp.where(core == 0, first, second)
    away = jnp.where(core == 0, second, first)
    return own, flip(away, count, 1), seen


def local(
    asking_matrix,
    matching_key_matrix,
    carried_value_matrix,
    silu_switch_argument,
    duality_source_matrix,
    storing_direction_matrix,
    fetching_direction_matrix,
    duality_kernel_coefficients,
    storing_kernel_coefficients,
    fetching_kernel_coefficients,
    raw_increment_lengths,
    logarithmic_fading_speeds,
    token_fading_spikes,
    absorber_score_vector,
    cluster_scaling_factor,
    final_mapping_matrix,
):
    rows = asking_matrix.shape[0]
    me = lax.axis_index("sp")
    count = lax.axis_size("sp")
    tps = lax.axis_size("tp")
    cols = duality_source_matrix.shape[1]
    wide = storing_direction_matrix.shape[1]
    heads = cols // SSD_HEAD
    sds = jax.ShapeDtypeStruct

    raw = (duality_source_matrix, storing_direction_matrix, fetching_direction_matrix)
    to_pair, to_outer = edges(raw)
    pair_edge = flip(to_pair, count, 1)
    outer_edge = outer(to_outer, count)

    span = final_mapping_matrix.shape[2]
    fast = tps == 2 and span % 128 == 0 and count == 16
    shared = [1, 4] if fast else [1]
    bits = []
    bit = count // 2
    while bit >= 2:
        if bit not in shared:
            bits.append(bit)
        bit //= 2

    def gather(piece):
        shards = {0: piece}
        for bit in bits:
            for mask in list(shards):
                shards[mask ^ bit] = flip(shards[mask], count, bit)
        return shards

    halves = [gather(final_mapping_matrix[0])]
    masks = sorted(halves[0])

    keep, send, read, inner, expl = call(
        block_kernel,
        [
            sds((2 * STATE + EDGE, cols // 2), BF16),
            sds((2 * STATE + EDGE, cols // 2), BF16),
            sds((rows, wide), BF16),
            sds((rows, cols), F32),
            sds((rows, 2 * heads), F32),
        ],
        [
            *raw,
            pair_edge,
            outer_edge,
            duality_kernel_coefficients,
            storing_kernel_coefficients,
            fetching_kernel_coefficients,
            raw_increment_lengths.reshape(2 * heads, rows),
            logarithmic_fading_speeds,
            token_fading_spikes.reshape(2 * heads, rows),
        ],
        flops=4 * 10**9,
        scratch=[
            pltpu.VMEM((rows + 2 * EDGE, max(cols, wide)), F32),
            pltpu.VMEM((rows, cols), BF16),
            pltpu.VMEM((rows, wide), BF16),
        ],
    )
    own_state, got_state, seen = exchange_states(keep, send, count, me)
    later, weights, matching_key, carried_value = lax.optimization_barrier(
        (me, final_mapping_matrix, matching_key_matrix, carried_value_matrix, seen)
    )[:4]
    right_rows = weights[1]
    middle = right_rows.shape[0] // 2
    halves += [gather(right_rows[:middle]), gather(right_rows[middle:])]
    pairs = jnp.concatenate([matching_key, carried_value], axis=1)
    pair_kv = flip(pairs, count, 1)
    outer_kv = outer(pairs, count)

    halfway = HEAD // 2
    spacing = ROTARY_BASE ** (-jnp.arange(halfway, dtype=F32) * 2.0 / HEAD)
    places = ((later - 1) * rows + jnp.arange(3 * rows, dtype=jnp.int32)).astype(F32)
    angles = places[:, None] * spacing[None, :]
    cosine = jnp.cos(angles)
    sine = jnp.sin(angles)
    cosine = jnp.concatenate([cosine, cosine], axis=1)
    sine = jnp.concatenate([-sine, sine], axis=1)
    (attended,) = call(
        attend_kernel,
        [sds(asking_matrix.shape, BF16)],
        [
            absorber_score_vector,
            asking_matrix,
            matching_key_matrix,
            carried_value_matrix,
            pair_kv,
            outer_kv,
            cosine,
            sine,
        ],
        flops=3 * 10**9,
        scalars=1,
    )

    def spread_rows(a):
        blocks = [a]
        for bit in reversed(shared):
            blocks += [flip(b, count, bit) for b in blocks]
        return blocks

    attended_blocks = spread_rows(attended)

    (normed,) = call(
        finish_kernel,
        [sds((rows, cols), BF16)],
        [
            inner,
            read,
            expl,
            own_state,
            got_state,
            silu_switch_argument,
            cluster_scaling_factor.reshape(1, cols),
        ],
        flops=3 * 10**9,
    )
    normed_blocks = spread_rows(normed)
    if fast:
        group = [0, 4, 1, 5]
        width = span * len(masks)
        sizes = (len(group), len(masks))
        flops = 2 * len(group) * rows * cols * width
        (early,) = call(
            functools.partial(first_kernel, sizes),
            [sds((len(group) * rows, width), F32)],
            [*attended_blocks, *[halves[0][m] for m in masks]],
            flops=flops,
        )
        pieces = []
        cut = len(masks)
        for turn, chosen in enumerate((masks,)):
            wide_part = span * len(chosen)
            outs = call(
                functools.partial(second_kernel, (len(group), len(chosen), turn * span * cut)),
                [sds((rows // 2, wide_part), BF16)] * (2 * len(group)),
                [
                    early,
                    *normed_blocks,
                    *[halves[1][m] for m in chosen],
                    *[halves[2][m] for m in chosen],
                ],
                flops=flops,
            )
            for i, m in enumerate(group):
                kept, gone = outs[2 * i], outs[2 * i + 1]
                pieces.append(kept if m == 0 else flip(kept, count, m))
                pieces.append(cross(gone, count, m))
        (out,) = call(
            functools.partial(place_kernel, group, masks, span),
            [sds((rows // 2, span * count), BF16)],
            pieces,
            flops=10**6,
        )
        return out

    attended_pair = attended_blocks[1]
    normed_pair = normed_blocks[1]
    shards = {
        m: jnp.stack([halves[0][m], jnp.concatenate([halves[1][m], halves[2][m]])]) for m in masks
    }
    left = jnp.concatenate(
        [
            jnp.concatenate([attended, normed], axis=1),
            jnp.concatenate([attended_pair, normed_pair], axis=1),
        ],
        axis=0,
    )
    stacked = jnp.concatenate([shards[m] for m in masks], axis=2).reshape(
        -1, span * len(masks)
    )
    partial = jnp.dot(left, stacked, preferred_element_type=F32).astype(BF16)
    partial = partial.reshape(2, tps, rows // tps, -1)
    summed = lax.psum_scatter(partial, "tp", scatter_dimension=1, tiled=True)
    summed = summed.reshape(2, rows // tps, len(masks), span)
    own, away = summed[0], flip(summed[1], count, 1)
    full = [None] * count
    for j, m in enumerate(masks):
        full[m] = own[:, j]
        full[m ^ 1] = away[:, j]
    full = jnp.stack(full, axis=0)
    bit = 1
    while bit < count:
        seen = full.reshape(count // (2 * bit), 2, bit, rows // tps, span)
        full = jnp.where((me & bit) != 0, seen[:, ::-1], seen).reshape(full.shape)
        bit *= 2
    return jnp.moveaxis(full, 0, 1).reshape(rows // tps, count * span)


def solution(mesh):
    in_specs = (
        P("sp", "tp"),
        P("sp", "tp"),
        P("sp", "tp"),
        P("sp", "tp"),
        P("sp", "tp"),
        P("sp", "tp"),
        P("sp", "tp"),
        P(None, "tp"),
        P(None, "tp"),
        P(None, "tp"),
        P(None, "tp", "sp"),
        P(None, "tp"),
        P(None, "tp", "sp"),
        P("tp"),
        P("tp"),
        P(None, "tp", "sp"),
    )
    out_specs = P(("sp", "tp"), None)

    return jax.shard_map(local, mesh=mesh, in_specs=in_specs, out_specs=out_specs, check_vma=False)
```

```python
import functools

import jax
import jax.numpy as jnp
from jax import lax
from jax.experimental import pallas as pl
from jax.experimental.pallas import tpu as pltpu
from jax.sharding import PartitionSpec as P


HEAD = 128
SSD_HEAD = 64
STATE = 128
CONV = 5
WINDOW = 128
EDGE = 16

ROTARY_BASE = 500000.0
EPSILON = 1e-06
HIGHEST = lax.Precision.HIGHEST
F32 = jnp.float32
BF16 = jnp.bfloat16
VMEM = pl.BlockSpec(memory_space=pltpu.VMEM)
SMEM = pl.BlockSpec(memory_space=pltpu.SMEM)


LIMIT = 16 * 2**20
STAGGERED = ()
PARTS = 1
LATE = 2


def call(kernel, outs, ins, flops, scratch=(), scalars=0):
    moved = sum(a.size * a.dtype.itemsize for a in list(ins) + list(outs))
    return pl.pallas_call(
        kernel,
        out_shape=outs,
        in_specs=[SMEM] * scalars + [VMEM] * (len(ins) - scalars),
        out_specs=[VMEM] * len(outs),
        scratch_shapes=list(scratch),
        cost_estimate=pl.CostEstimate(flops=flops, bytes_accessed=moved, transcendentals=0),
        compiler_params=pltpu.CompilerParams(vmem_limit_bytes=LIMIT),
    )(*ins)


def nn(a, b, precision=None):
    return lax.dot_general(
        a, b, (((1,), (0,)), ((), ())), precision=precision, preferred_element_type=F32
    )


def nt(a, b, precision=None):
    return lax.dot_general(
        a, b, (((1,), (1,)), ((), ())), precision=precision, preferred_element_type=F32
    )


def silu(v):
    return v / (1.0 + jnp.exp(-v))


def head_spread(heads, cols):
    head = lax.broadcasted_iota(jnp.int32, (heads, cols), 0)
    col = lax.broadcasted_iota(jnp.int32, (heads, cols), 1)
    return jnp.where(col // SSD_HEAD == head, 1.0, 0.0).astype(F32)


def block_kernel(
    x_ref,
    w_ref,
    r_ref,
    pair_ref,
    outer_ref,
    tx_ref,
    tw_ref,
    tr_ref,
    inc_ref,
    fade_ref,
    spike_ref,
    keep_ref,
    send_ref,
    read_ref,
    y_ref,
    expl_ref,
    line,
    xs,
    ws,
):
    rows, cols = x_ref.shape
    wide = w_ref.shape[1]
    core = lax.axis_index("sp") & 1
    heads = cols // SSD_HEAD
    groups = wide // STATE
    per = heads // groups
    margin = CONV // 2
    start = 0
    for src, taps, dst in ((x_ref, tx_ref, xs), (w_ref, tw_ref, ws), (r_ref, tr_ref, read_ref)):
        span = src.shape[1]
        pair = pair_ref[:, start : start + span].astype(F32)
        outer = outer_ref[:, start : start + span].astype(F32)
        line[0:EDGE, 0:span] = jnp.where(core == 0, outer, pair)
        line[EDGE : EDGE + rows, 0:span] = src[...].astype(F32)
        line[EDGE + rows : 2 * EDGE + rows, 0:span] = jnp.where(core == 0, pair, outer)
        step = min(span, 256)
        for at in range(0, span, step):
            total = jnp.zeros((rows, step), F32)
            for k in range(CONV):
                low = EDGE - margin + k
                total = total + line[low : low + rows, at : at + step] * taps[
                    k : k + 1, at : at + step
                ].astype(F32)
            dst[:, at : at + step] = silu(total).astype(BF16)
        start += span

    steps = jax.nn.softplus(inc_ref[...])
    square = lax.broadcasted_iota(jnp.int32, (heads, heads), 0)
    square = square == lax.broadcasted_iota(jnp.int32, (heads, heads), 1)
    rates = jnp.concatenate(
        [
            jnp.sum(jnp.where(square, jnp.exp(fade_ref[d : d + 1, :]), 0.0), axis=1, keepdims=True)
            for d in range(2)
        ],
        axis=0,
    )
    logs = -rates * steps + spike_ref[...]
    first = lax.broadcasted_iota(jnp.int32, (rows, rows), 0)
    second = lax.broadcasted_iota(jnp.int32, (rows, rows), 1)
    lower = first >= second
    upper = first <= second
    run_f = nn(logs[0:heads], jnp.where(upper, 1.0, 0.0), HIGHEST)
    run_b = nn(logs[heads : 2 * heads], jnp.where(lower, 1.0, 0.0), HIGHEST)
    tall = jnp.concatenate([run_f, run_b], axis=0).T
    grown = jnp.exp(tall)
    coarse = grown.astype(BF16)
    fine = (grown - coarse.astype(F32)).astype(BF16)
    expl_ref[...] = jnp.concatenate(
        [coarse[:, 0:heads], fine[:, 0:heads], coarse[:, heads:], fine[:, heads:]], axis=1
    )
    tot_f = run_f[:, rows - 1 : rows]
    tot_b = run_b[:, 0:1]
    end_f = jnp.exp(tot_f - run_f) * steps[0:heads]
    end_b = jnp.exp(tot_b - run_b) * steps[heads : 2 * heads]

    spread = head_spread(heads, cols)
    tot = jnp.exp(jnp.concatenate([tall[rows - 1 : rows, 0:heads], tall[0:1, heads:]], axis=0))
    tot = nn(tot, spread, HIGHEST)
    high = tot.astype(BF16)
    low = (tot - high.astype(F32)).astype(BF16)
    half = cols // 2
    tail = jnp.concatenate(
        [high.astype(F32), low.astype(F32), jnp.zeros((EDGE - 4, cols), F32)], axis=0
    ).astype(BF16)
    bodies = []
    for g in range(groups):
        wg = ws[:, g * STATE : (g + 1) * STATE]
        rg = read_ref[:, g * STATE : (g + 1) * STATE]
        affinity = nt(rg, wg)
        turned = wg.astype(F32).T
        fresh = []
        for j in range(per):
            h = g * per + j
            at = h * SSD_HEAD
            ahead = jnp.exp(
                jnp.where(lower, tall[:, h : h + 1] - run_f[h : h + 1, :], -jnp.inf)
            ) * steps[h : h + 1, :]
            back = jnp.exp(
                jnp.where(
                    upper, tall[:, heads + h : heads + h + 1] - run_b[h : h + 1, :], -jnp.inf
                )
            ) * steps[heads + h : heads + h + 1, :]
            mixed = (affinity * (ahead + back)).astype(BF16)
            grow_f = (turned * end_f[h : h + 1, :]).astype(BF16)
            grow_b = (turned * end_b[h : h + 1, :]).astype(BF16)
            got = nn(jnp.concatenate([mixed, grow_f, grow_b], axis=0), xs[:, at : at + SSD_HEAD])
            y_ref[:, at : at + SSD_HEAD] = got[0:rows]
            fresh.append(got[rows : rows + 2 * STATE].astype(BF16))
        bodies.append(jnp.concatenate(fresh, axis=1))
    whole = jnp.concatenate([jnp.concatenate(bodies, axis=1), tail], axis=0)
    near = whole[:, :half].astype(F32)
    away = whole[:, half:].astype(F32)
    keep_ref[...] = jnp.where(core == 0, near, away).astype(BF16)
    send_ref[...] = jnp.where(core == 0, away, near).astype(BF16)


def attend_kernel(
    sink, q_ref, k_ref, v_ref, pair_ref, outer_ref, cos_ref, sin_ref, out_ref
):
    rows = q_ref.shape[0]
    me = lax.axis_index("sp")
    last = lax.axis_size("sp") - 1
    kv = k_ref.shape[1] // HEAD
    sharing = q_ref.shape[1] // k_ref.shape[1]
    wide = k_ref.shape[1]

    def turn(m, low):
        m = m.astype(F32)
        half = HEAD // 2
        other = jnp.concatenate([m[:, half:], m[:, :half]], axis=1)
        high = low + m.shape[0]
        return (m * cos_ref[low:high, :] + other * sin_ref[low:high, :]).astype(BF16)

    within = lax.broadcasted_iota(jnp.int32, (rows, 3 * rows), 0)
    across = lax.broadcasted_iota(jnp.int32, (rows, 3 * rows), 1)
    far = across - rows - within
    allowed = (far <= WINDOW) & (far >= -WINDOW)
    allowed = allowed & ((across >= rows) | (me > 0))
    allowed = allowed & ((across < 2 * rows) | (me < last))
    even = (me & 1) == 0
    for g in range(kv):
        at = g * HEAD
        near = [
            (pair_ref[:, a : a + HEAD].astype(F32), outer_ref[:, a : a + HEAD].astype(F32))
            for a in (at, wide + at)
        ]
        before = [jnp.where(even, o, p) for p, o in near]
        after = [jnp.where(even, p, o) for p, o in near]
        keys = jnp.concatenate(
            [
                turn(before[0], 0),
                turn(k_ref[:, at : at + HEAD], rows),
                turn(after[0], 2 * rows),
            ],
            axis=0,
        )
        values = jnp.concatenate(
            [
                before[1].astype(BF16),
                v_ref[:, at : at + HEAD],
                after[1].astype(BF16),
            ],
            axis=0,
        )
        for j in range(sharing):
            h = g * sharing + j
            query = turn(q_ref[:, h * HEAD : (h + 1) * HEAD], rows)
            scores = nt(query, keys) * HEAD ** (-0.5)
            scores = jnp.where(allowed, scores, -jnp.inf)
            top = jnp.maximum(jnp.max(scores, axis=1, keepdims=True), sink[h])
            weights = jnp.exp(scores - top)
            total = jnp.sum(weights, axis=1, keepdims=True) + jnp.exp(sink[h] - top)
            chance = (weights / total).astype(BF16)
            out_ref[:, h * HEAD : (h + 1) * HEAD] = nn(chance, values).astype(BF16)


def finish_kernel(y_ref, read_ref, expl_ref, own_ref, got_ref, gate_ref, gain_ref, out_ref):
    _, cols = y_ref.shape
    core = lax.axis_index("sp") & 1
    wide = read_ref.shape[1]
    heads = cols // SSD_HEAD
    groups = wide // STATE
    size = cols // groups
    half = cols // 2
    spread = head_spread(heads, cols).astype(BF16)
    spread = jnp.concatenate([spread, spread], axis=0)
    for g in range(groups):
        at = g * size
        rg = read_ref[:, g * STATE : (g + 1) * STATE]
        pieces = []
        for low in range(at, at + size, min(size, half)):
            span = min(size, half)
            side = low // half
            off = low - side * half
            mine = core == side
            pieces.append(
                jnp.where(
                    mine,
                    own_ref[:, off : off + span].astype(F32),
                    got_ref[:, off : off + span].astype(F32),
                ).astype(BF16)
            )
        states = pieces[0] if len(pieces) == 1 else jnp.concatenate(pieces, axis=1)
        local = spread[:, at : at + size]
        fade_f = nn(expl_ref[:, 0 : 2 * heads], local)
        fade_b = nn(expl_ref[:, 2 * heads : 4 * heads], local)
        both = (
            y_ref[:, at : at + size]
            + fade_f * nn(rg, states[0:STATE])
            + fade_b * nn(rg, states[STATE : 2 * STATE])
        )
        gated = both * silu(gate_ref[:, at : at + size].astype(F32))
        mean = jnp.sum(gated * gated, axis=1, keepdims=True) * (1.0 / size)
        out_ref[:, at : at + size] = (
            gated * lax.rsqrt(mean + EPSILON) * gain_ref[:, at : at + size]
        ).astype(BF16)


def first_kernel(count, *refs):
    lefts = refs[: count[0]]
    shards = refs[count[0] : count[0] + count[1]]
    out_ref = refs[-1]
    left = jnp.concatenate([a[...] for a in lefts], axis=0)
    at = 0
    for shard in shards:
        span = shard.shape[1]
        out_ref[:, at : at + span] = nn(left, shard[...])
        at += span


def second_kernel(count, base, sum_ref, *refs):
    place = lax.axis_index("tp")
    blocks, shards = count
    lefts = refs[:blocks]
    pieces = refs[blocks : blocks + 2 * shards]
    outs = refs[blocks + 2 * shards : -3]
    held, early, sems = refs[-3:]
    rows = lefts[0].shape[0]
    half = rows // 2
    deep, span = pieces[0].shape
    whole = deep + pieces[shards].shape[0]
    copies = []
    for j in range(shards):
        for k in range(2):
            i = 2 * j + k
            copies.append(
                pltpu.make_async_copy(
                    pieces[k * shards + j],
                    held.at[j, 0:deep] if k == 0 else held.at[j, deep:whole],
                    sems.at[i],
                )
            )
        at = j * span
        copies.append(
            pltpu.make_async_copy(
                sum_ref.at[:, base + at : base + at + span], early.at[j], sems.at[2 * shards + j]
            )
        )
    for copy in copies:
        copy.start()
    left = jnp.concatenate([a[...] for a in lefts], axis=0)
    for j in range(shards):
        at = j * span
        for copy in copies[3 * j : 3 * j + 3]:
            copy.wait()
        total = early[j] + nn(left, held[j])
        for i in range(blocks):
            top = total[i * rows : i * rows + half]
            low = total[i * rows + half : (i + 1) * rows]
            outs[2 * i][:, at : at + span] = jnp.where(place == 0, top, low).astype(BF16)
            outs[2 * i + 1][:, at : at + span] = jnp.where(place == 0, low, top).astype(BF16)


def place_kernel(group, parts, span, *refs):
    me = lax.axis_index("sp")
    out_ref = refs[-1]
    at = 0
    for masks in parts:
        for block in group:
            for j, mask in enumerate(masks):
                low = j * span
                to = pl.multiple_of((me ^ (block ^ mask)) * span, span)
                out_ref[:, pl.ds(to, span)] = (
                    refs[at][:, low : low + span].astype(F32)
                    + refs[at + 1][:, low : low + span].astype(F32)
                ).astype(BF16)
            at += 2


def edge_kernel(*refs):
    even = (lax.axis_index("sp") & 1) == 0
    start = 0
    for i in range(0, 6, 2):
        lead = refs[i][...].astype(F32)
        tail = refs[i + 1][...].astype(F32)
        span = lead.shape[1]
        refs[6][:, start : start + span] = jnp.where(even, tail, lead).astype(BF16)
        refs[7][:, start : start + span] = jnp.where(even, lead, tail).astype(BF16)
        start += span


def edges(raw):
    specs = []
    for a in raw:
        end = a.shape[0] // EDGE - 1
        specs.append(pl.BlockSpec((EDGE, a.shape[1]), lambda i: (0, 0)))
        specs.append(pl.BlockSpec((EDGE, a.shape[1]), lambda i, end=end: (end, 0)))
    width = sum(a.shape[1] for a in raw)
    return pl.pallas_call(
        edge_kernel,
        grid=(1,),
        out_shape=[jax.ShapeDtypeStruct((EDGE, width), BF16)] * 2,
        in_specs=specs,
        out_specs=[pl.BlockSpec((EDGE, width), lambda i: (0, 0))] * 2,
        compiler_params=pltpu.CompilerParams(vmem_limit_bytes=LIMIT),
        name="edges",
    )(*[a for a in raw for _ in range(2)])


def join_kernel(keep_ref, got_ref, out_ref):
    even = (lax.axis_index("sp") & 1) == 0
    end = 2 * STATE

    def load(low, high):
        mine = keep_ref[low:high, :].astype(F32)
        theirs = got_ref[low:high, :].astype(F32)
        return jnp.where(even, mine, theirs), jnp.where(even, theirs, mine)

    low, high = load(end, end + EDGE)
    low = low[0:2] + low[2:4]
    high = high[0:2] + high[2:4]
    fades = low * high
    top = fades.astype(BF16).astype(F32)
    rest = fades - top
    out_ref[end : end + EDGE, :] = jnp.concatenate(
        [top, rest, jnp.zeros((EDGE - 4, top.shape[1]), F32)], axis=0
    ).astype(BF16)
    a, b = load(0, STATE)
    out_ref[0:STATE, :] = (a * high[0:1] + b).astype(BF16)
    a, b = load(STATE, end)
    out_ref[STATE:end, :] = (b * low[1:2] + a).astype(BF16)


def flip(a, count, mask):
    return lax.ppermute(a, "sp", [(i, i ^ mask) for i in range(count)])


def outer(a, count):
    pairs = [(i, i + 1) for i in range(1, count - 1, 2)]
    return lax.ppermute(a, "sp", pairs + [(j, i) for i, j in pairs])


def cross(a, count, mask):
    return lax.ppermute(
        a,
        ("sp", "tp"),
        [(2 * i + j, 2 * (i ^ mask) + 1 - j) for i in range(count) for j in range(2)],
    )


def join_pair(keep, got):
    (payload,) = call(
        join_kernel, [jax.ShapeDtypeStruct(keep.shape, BF16)], [keep, got], flops=10**6
    )
    return payload


def tails(ref):
    end = 2 * STATE
    tail = ref[end : end + EDGE, :].astype(F32)
    return tail[0:2] + tail[2:4]


def merge_kernel(bit, first, closing, *refs):
    me = lax.axis_index("sp")
    upper = (me & bit) != 0
    end = 2 * STATE
    own_ref, other_ref = refs[0], refs[1]
    carry_ref = None if first else refs[2]
    out_ref, next_ref = refs[-2:]
    mine, theirs = tails(own_ref), tails(other_ref)
    own_f, own_b = own_ref[0:STATE, :].astype(F32), own_ref[STATE:end, :].astype(F32)
    far_f, far_b = other_ref[0:STATE, :].astype(F32), other_ref[STATE:end, :].astype(F32)
    zero = jnp.zeros_like(own_f)
    if first:
        gap_f = gap_b = jnp.ones_like(mine[0:1])
        next_ref[0:STATE, :] = jnp.where(upper, far_f, zero)
        next_ref[STATE:end, :] = jnp.where(upper, zero, far_b)
    else:
        gap_f = carry_ref[end : end + 1, :]
        gap_b = carry_ref[end + 1 : end + 2, :]
        next_ref[0:STATE, :] = carry_ref[0:STATE, :] + jnp.where(upper, far_f * gap_f, zero)
        next_ref[STATE:end, :] = carry_ref[STATE:end, :] + jnp.where(upper, zero, far_b * gap_b)
    gap_f = jnp.where(upper, gap_f * theirs[0:1], gap_f)
    gap_b = jnp.where(upper, gap_b, gap_b * theirs[1:2])
    pad = jnp.zeros((6, gap_f.shape[1]), F32)
    next_ref[end : end + 8, :] = jnp.concatenate([gap_f, gap_b, pad], axis=0)
    low_f, high_f = jnp.where(upper, far_f, own_f), jnp.where(upper, own_f, far_f)
    low_b, high_b = jnp.where(upper, far_b, own_b), jnp.where(upper, own_b, far_b)
    low, high = jnp.where(upper, theirs, mine), jnp.where(upper, mine, theirs)
    total_f = low_f * high[0:1] + high_f
    total_b = high_b * low[1:2] + low_b
    if closing:
        out_ref[...] = jnp.where((me & (2 * bit)) != 0, total_b, total_f).astype(BF16)
        return
    out_ref[0:STATE, :] = total_f.astype(BF16)
    out_ref[STATE:end, :] = total_b.astype(BF16)
    fades = low * high
    top = fades.astype(BF16).astype(F32)
    pad = jnp.zeros((EDGE - 4, fades.shape[1]), F32)
    out_ref[end : end + EDGE, :] = jnp.concatenate([top, fades - top, pad], axis=0).astype(BF16)


def close_kernel(bit, other_ref, carry_ref, keep_ref, got_ref, own_ref, away_ref):
    me = lax.axis_index("sp")
    upper = (me & bit) != 0
    even = (me & 1) == 0
    end = 2 * STATE
    other = other_ref[...].astype(F32)
    zero = jnp.zeros_like(other)
    gap_f = carry_ref[end : end + 1, :]
    gap_b = carry_ref[end + 1 : end + 2, :]
    into_f = carry_ref[0:STATE, :] + jnp.where(upper, other * gap_f, zero)
    into_b = carry_ref[STATE:end, :] + jnp.where(upper, zero, other * gap_b)
    mine, theirs = tails(keep_ref), tails(got_ref)
    keep_f, keep_b = keep_ref[0:STATE, :].astype(F32), keep_ref[STATE:end, :].astype(F32)
    got_f, got_b = got_ref[0:STATE, :].astype(F32), got_ref[STATE:end, :].astype(F32)
    low_f = jnp.where(even, keep_f, got_f)
    high_b = jnp.where(even, got_b, keep_b)
    low, high = jnp.where(even, mine, theirs), jnp.where(even, theirs, mine)
    second_f = into_f * low[0:1] + low_f
    first_b = into_b * high[1:2] + high_b
    own_ref[0:STATE, :] = jnp.where(even, into_f, second_f).astype(BF16)
    own_ref[STATE:end, :] = jnp.where(even, first_b, into_b).astype(BF16)
    away_ref[0:STATE, :] = jnp.where(even, second_f, into_f).astype(BF16)
    away_ref[STATE:end, :] = jnp.where(even, into_b, first_b).astype(BF16)


def exchange_states(keep, send, count):
    half = keep.shape[1]
    sds = jax.ShapeDtypeStruct
    got = flip(send, count, 1)
    seen = payload = join_pair(keep, got)
    carry = None
    bit = 2
    while 2 * bit < count:
        other = flip(payload, count, bit)
        closing = 4 * bit >= count
        payload, carry = call(
            functools.partial(merge_kernel, bit, carry is None, closing),
            [
                sds((STATE, half) if closing else keep.shape, BF16),
                sds((2 * STATE + 8, half), F32),
            ],
            [payload, other] + ([] if carry is None else [carry]),
            flops=10**6,
        )
        bit *= 2
    other = flip(payload, count, bit)
    own, away = call(
        functools.partial(close_kernel, bit),
        [sds((2 * STATE, half), BF16)] * 2,
        [other, carry, keep, got],
        flops=10**6,
    )
    return own, flip(away, count, 1), seen


def local(
    asking_matrix,
    matching_key_matrix,
    carried_value_matrix,
    silu_switch_argument,
    duality_source_matrix,
    storing_direction_matrix,
    fetching_direction_matrix,
    duality_kernel_coefficients,
    storing_kernel_coefficients,
    fetching_kernel_coefficients,
    raw_increment_lengths,
    logarithmic_fading_speeds,
    token_fading_spikes,
    absorber_score_vector,
    cluster_scaling_factor,
    final_mapping_matrix,
):
    rows = asking_matrix.shape[0]
    me = lax.axis_index("sp")
    count = lax.axis_size("sp")
    tps = lax.axis_size("tp")
    cols = duality_source_matrix.shape[1]
    wide = storing_direction_matrix.shape[1]
    heads = cols // SSD_HEAD
    sds = jax.ShapeDtypeStruct

    raw = (duality_source_matrix, storing_direction_matrix, fetching_direction_matrix)
    to_pair, to_outer = edges(raw)
    pair_edge = flip(to_pair, count, 1)
    outer_edge = outer(to_outer, count)

    span = final_mapping_matrix.shape[2]
    fast = tps == 2 and span % 128 == 0 and count == 16
    shared = [1, 4] if fast else [1]
    bits = []
    bit = count // 2
    while bit >= 2:
        if bit not in shared:
            bits.append(bit)
        bit //= 2

    def turns(a):
        got = []
        for turn in range(2):
            pairs = [(i, i ^ 8) for i in range(count) if ((i >> 2) & 1) == turn]
            got.append(lax.ppermute(a, "sp", pairs))
        return jnp.where((me & 4) == 0, got[0], got[1])

    def gather(part, piece):
        shards = {0: piece}
        for bit in bits:
            for mask in list(shards):
                if fast and bit == 8 and part in STAGGERED:
                    shards[mask ^ bit] = turns(shards[mask])
                else:
                    shards[mask ^ bit] = flip(shards[mask], count, bit)
        return shards

    deepest = final_mapping_matrix.shape[1]
    middle = deepest - deepest // LATE
    halves = [gather(0, final_mapping_matrix[0])]
    masks = sorted(halves[0])

    keep, send, read, inner, expl = call(
        block_kernel,
        [
            sds((2 * STATE + EDGE, cols // 2), BF16),
            sds((2 * STATE + EDGE, cols // 2), BF16),
            sds((rows, wide), BF16),
            sds((rows, cols), F32),
            sds((rows, 4 * heads), BF16),
        ],
        [
            *raw,
            pair_edge,
            outer_edge,
            duality_kernel_coefficients,
            storing_kernel_coefficients,
            fetching_kernel_coefficients,
            raw_increment_lengths.reshape(2 * heads, rows),
            logarithmic_fading_speeds,
            token_fading_spikes.reshape(2 * heads, rows),
        ],
        flops=4 * 10**9,
        scratch=[
            pltpu.VMEM((rows + 2 * EDGE, max(cols, wide)), F32),
            pltpu.VMEM((rows, cols), BF16),
            pltpu.VMEM((rows, wide), BF16),
        ],
    )
    own_state, got_state, seen = exchange_states(keep, send, count)
    later, weights, _, _ = lax.optimization_barrier(
        (me, final_mapping_matrix, matching_key_matrix, carried_value_matrix, seen)
    )[:4]
    halves += [gather(1, weights[1, :middle]), gather(2, weights[1, middle:])]
    pairs = jnp.concatenate([matching_key_matrix, carried_value_matrix], axis=1)
    pair_kv = flip(pairs, count, 1)
    outer_kv = outer(pairs, count)

    halfway = HEAD // 2
    spacing = ROTARY_BASE ** (-jnp.arange(halfway, dtype=F32) * 2.0 / HEAD)
    places = ((later - 1) * rows + jnp.arange(3 * rows, dtype=jnp.int32)).astype(F32)
    angles = places[:, None] * spacing[None, :]
    cosine = jnp.cos(angles)
    sine = jnp.sin(angles)
    cosine = jnp.concatenate([cosine, cosine], axis=1)
    sine = jnp.concatenate([-sine, sine], axis=1)
    (attended,) = call(
        attend_kernel,
        [sds(asking_matrix.shape, BF16)],
        [
            absorber_score_vector,
            asking_matrix,
            matching_key_matrix,
            carried_value_matrix,
            pair_kv,
            outer_kv,
            cosine,
            sine,
        ],
        flops=3 * 10**9,
        scalars=1,
    )

    def spread_rows(a):
        blocks = [a]
        for bit in reversed(shared):
            blocks += [flip(b, count, bit) for b in blocks]
        return blocks

    attended_blocks = spread_rows(attended)

    (normed,) = call(
        finish_kernel,
        [sds((rows, cols), BF16)],
        [
            inner,
            read,
            expl,
            own_state,
            got_state,
            silu_switch_argument,
            cluster_scaling_factor.reshape(1, cols),
        ],
        flops=3 * 10**9,
    )
    normed_blocks = spread_rows(normed)
    if fast:
        group = [0, 4, 1, 5]
        width = span * len(masks)
        sizes = (len(group), len(masks))
        flops = 2 * len(group) * rows * cols * width
        (early,) = call(
            functools.partial(first_kernel, sizes),
            [sds((len(group) * rows, width), F32)],
            [*attended_blocks, *[halves[0][m] for m in masks]],
            flops=flops,
        )
        pieces = []
        cut = len(masks) // PARTS
        parted = [masks[i : i + cut] for i in range(0, len(masks), cut)]
        for turn, chosen in enumerate(parted):
            wide_part = span * len(chosen)
            parts = [halves[1][m] for m in chosen] + [halves[2][m] for m in chosen]
            anywhere = pl.BlockSpec(memory_space=pl.ANY)
            deep = parts[0].shape[0] + parts[-1].shape[0]
            outs = pl.pallas_call(
                functools.partial(second_kernel, (len(group), len(chosen)), turn * cut * span),
                out_shape=[sds((rows // 2, wide_part), BF16)] * (2 * len(group)),
                in_specs=[anywhere] + [VMEM] * len(group) + [anywhere] * len(parts),
                out_specs=[VMEM] * (2 * len(group)),
                scratch_shapes=[
                    pltpu.VMEM((len(chosen), deep, span), BF16),
                    pltpu.VMEM((len(chosen), len(group) * rows, span), F32),
                    pltpu.SemaphoreType.DMA((len(parts) + len(chosen),)),
                ],
                cost_estimate=pl.CostEstimate(
                    flops=flops // PARTS, bytes_accessed=6 * 2**20, transcendentals=0
                ),
                compiler_params=pltpu.CompilerParams(vmem_limit_bytes=LIMIT),
                name="second",
            )(early, *normed_blocks, *parts)
            for i, m in enumerate(group):
                kept, gone = outs[2 * i], outs[2 * i + 1]
                pieces.append(kept if m == 0 else flip(kept, count, m))
                pieces.append(cross(gone, count, m))
        (out,) = call(
            functools.partial(place_kernel, group, parted, span),
            [sds((rows // 2, span * count), BF16)],
            pieces,
            flops=10**6,
        )
        return out

    attended_pair = attended_blocks[1]
    normed_pair = normed_blocks[1]
    shards = {
        m: jnp.stack([halves[0][m], jnp.concatenate([halves[1][m], halves[2][m]])]) for m in masks
    }
    left = jnp.concatenate(
        [
            jnp.concatenate([attended, normed], axis=1),
            jnp.concatenate([attended_pair, normed_pair], axis=1),
        ],
        axis=0,
    )
    stacked = jnp.concatenate([shards[m] for m in masks], axis=2).reshape(
        -1, span * len(masks)
    )
    partial = jnp.dot(left, stacked, preferred_element_type=F32).astype(BF16)
    partial = partial.reshape(2, tps, rows // tps, -1)
    summed = lax.psum_scatter(partial, "tp", scatter_dimension=1, tiled=True)
    summed = summed.reshape(2, rows // tps, len(masks), span)
    own, away = summed[0], flip(summed[1], count, 1)
    full = [None] * count
    for j, m in enumerate(masks):
        full[m] = own[:, j]
        full[m ^ 1] = away[:, j]
    full = jnp.stack(full, axis=0)
    bit = 1
    while bit < count:
        seen = full.reshape(count // (2 * bit), 2, bit, rows // tps, span)
        full = jnp.where((me & bit) != 0, seen[:, ::-1], seen).reshape(full.shape)
        bit *= 2
    return jnp.moveaxis(full, 0, 1).reshape(rows // tps, count * span)


def solution(mesh):
    in_specs = (
        P("sp", "tp"),
        P("sp", "tp"),
        P("sp", "tp"),
        P("sp", "tp"),
        P("sp", "tp"),
        P("sp", "tp"),
        P("sp", "tp"),
        P(None, "tp"),
        P(None, "tp"),
        P(None, "tp"),
        P(None, "tp", "sp"),
        P(None, "tp"),
        P(None, "tp", "sp"),
        P("tp"),
        P("tp"),
        P(None, "tp", "sp"),
    )
    out_specs = P(("sp", "tp"), None)

    return jax.shard_map(local, mesh=mesh, in_specs=in_specs, out_specs=out_specs, check_vma=False)
```

```python
import functools

import jax
import jax.numpy as jnp
from jax import lax
from jax.experimental import pallas as pl
from jax.experimental.pallas import tpu as pltpu
from jax.sharding import PartitionSpec as P


HEAD = 128
SSD_HEAD = 64
STATE = 128
CONV = 5
WINDOW = 128
EDGE = 16

ROTARY_BASE = 500000.0
EPSILON = 1e-06
HIGHEST = lax.Precision.HIGHEST
F32 = jnp.float32
BF16 = jnp.bfloat16
VMEM = pl.BlockSpec(memory_space=pltpu.VMEM)
SMEM = pl.BlockSpec(memory_space=pltpu.SMEM)


LIMIT = 16 * 2**20
STAGGERED = ()
PARTS = 1
LATE = 2


def call(kernel, outs, ins, flops, scratch=(), scalars=0):
    moved = sum(a.size * a.dtype.itemsize for a in list(ins) + list(outs))
    return pl.pallas_call(
        kernel,
        out_shape=outs,
        in_specs=[SMEM] * scalars + [VMEM] * (len(ins) - scalars),
        out_specs=[VMEM] * len(outs),
        scratch_shapes=list(scratch),
        cost_estimate=pl.CostEstimate(flops=flops, bytes_accessed=moved, transcendentals=0),
        compiler_params=pltpu.CompilerParams(vmem_limit_bytes=LIMIT),
    )(*ins)


def nn(a, b, precision=None):
    return lax.dot_general(
        a, b, (((1,), (0,)), ((), ())), precision=precision, preferred_element_type=F32
    )


def nt(a, b, precision=None):
    return lax.dot_general(
        a, b, (((1,), (1,)), ((), ())), precision=precision, preferred_element_type=F32
    )


def silu(v):
    return v / (1.0 + jnp.exp(-v))


def head_spread(heads, cols):
    head = lax.broadcasted_iota(jnp.int32, (heads, cols), 0)
    col = lax.broadcasted_iota(jnp.int32, (heads, cols), 1)
    return jnp.where(col // SSD_HEAD == head, 1.0, 0.0).astype(F32)


def block_kernel(
    x_ref,
    w_ref,
    r_ref,
    pair_ref,
    outer_ref,
    tx_ref,
    tw_ref,
    tr_ref,
    inc_ref,
    fade_ref,
    spike_ref,
    keep_ref,
    send_ref,
    read_ref,
    y_ref,
    expl_ref,
    line,
    xs,
    ws,
):
    rows, cols = x_ref.shape
    wide = w_ref.shape[1]
    core = lax.axis_index("sp") & 1
    heads = cols // SSD_HEAD
    groups = wide // STATE
    per = heads // groups
    margin = CONV // 2
    start = 0
    for src, taps, dst in ((x_ref, tx_ref, xs), (w_ref, tw_ref, ws), (r_ref, tr_ref, read_ref)):
        span = src.shape[1]
        pair = pair_ref[:, start : start + span].astype(F32)
        outer = outer_ref[:, start : start + span].astype(F32)
        line[0:EDGE, 0:span] = jnp.where(core == 0, outer, pair)
        line[EDGE : EDGE + rows, 0:span] = src[...].astype(F32)
        line[EDGE + rows : 2 * EDGE + rows, 0:span] = jnp.where(core == 0, pair, outer)
        step = min(span, 256)
        for at in range(0, span, step):
            total = jnp.zeros((rows, step), F32)
            for k in range(CONV):
                low = EDGE - margin + k
                total = total + line[low : low + rows, at : at + step] * taps[
                    k : k + 1, at : at + step
                ].astype(F32)
            dst[:, at : at + step] = silu(total).astype(BF16)
        start += span

    steps = jax.nn.softplus(inc_ref[...])
    square = lax.broadcasted_iota(jnp.int32, (heads, heads), 0)
    square = square == lax.broadcasted_iota(jnp.int32, (heads, heads), 1)
    rates = jnp.concatenate(
        [
            jnp.sum(jnp.where(square, jnp.exp(fade_ref[d : d + 1, :]), 0.0), axis=1, keepdims=True)
            for d in range(2)
        ],
        axis=0,
    )
    logs = -rates * steps + spike_ref[...]
    first = lax.broadcasted_iota(jnp.int32, (rows, rows), 0)
    second = lax.broadcasted_iota(jnp.int32, (rows, rows), 1)
    lower = first >= second
    upper = first <= second
    run_f = nn(logs[0:heads], jnp.where(upper, 1.0, 0.0), HIGHEST)
    run_b = nn(logs[heads : 2 * heads], jnp.where(lower, 1.0, 0.0), HIGHEST)
    tall = jnp.concatenate([run_f, run_b], axis=0).T
    grown = jnp.exp(tall)
    coarse = grown.astype(BF16)
    fine = (grown - coarse.astype(F32)).astype(BF16)
    expl_ref[...] = jnp.concatenate(
        [coarse[:, 0:heads], fine[:, 0:heads], coarse[:, heads:], fine[:, heads:]], axis=1
    )
    tot_f = run_f[:, rows - 1 : rows]
    tot_b = run_b[:, 0:1]
    end_f = jnp.exp(tot_f - run_f) * steps[0:heads]
    end_b = jnp.exp(tot_b - run_b) * steps[heads : 2 * heads]

    spread = head_spread(heads, cols)
    tot = jnp.exp(jnp.concatenate([tall[rows - 1 : rows, 0:heads], tall[0:1, heads:]], axis=0))
    tot = nn(tot, spread, HIGHEST)
    high = tot.astype(BF16)
    low = (tot - high.astype(F32)).astype(BF16)
    half = cols // 2
    tail = jnp.concatenate(
        [high.astype(F32), low.astype(F32), jnp.zeros((EDGE - 4, cols), F32)], axis=0
    ).astype(BF16)
    bodies = []
    for g in range(groups):
        wg = ws[:, g * STATE : (g + 1) * STATE]
        rg = read_ref[:, g * STATE : (g + 1) * STATE]
        affinity = nt(rg, wg)
        turned = wg.astype(F32).T
        fresh = []
        for j in range(per):
            h = g * per + j
            at = h * SSD_HEAD
            ahead = jnp.exp(
                jnp.where(lower, tall[:, h : h + 1] - run_f[h : h + 1, :], -jnp.inf)
            ) * steps[h : h + 1, :]
            back = jnp.exp(
                jnp.where(
                    upper, tall[:, heads + h : heads + h + 1] - run_b[h : h + 1, :], -jnp.inf
                )
            ) * steps[heads + h : heads + h + 1, :]
            mixed = (affinity * (ahead + back)).astype(BF16)
            grow_f = (turned * end_f[h : h + 1, :]).astype(BF16)
            grow_b = (turned * end_b[h : h + 1, :]).astype(BF16)
            got = nn(jnp.concatenate([mixed, grow_f, grow_b], axis=0), xs[:, at : at + SSD_HEAD])
            y_ref[:, at : at + SSD_HEAD] = got[0:rows]
            fresh.append(got[rows : rows + 2 * STATE].astype(BF16))
        bodies.append(jnp.concatenate(fresh, axis=1))
    whole = jnp.concatenate([jnp.concatenate(bodies, axis=1), tail], axis=0)
    near = whole[:, :half].astype(F32)
    away = whole[:, half:].astype(F32)
    keep_ref[...] = jnp.where(core == 0, near, away).astype(BF16)
    send_ref[...] = jnp.where(core == 0, away, near).astype(BF16)


def attend_kernel(
    sink, q_ref, k_ref, v_ref, pair_ref, outer_ref, cos_ref, sin_ref, out_ref
):
    rows = q_ref.shape[0]
    me = lax.axis_index("sp")
    last = lax.axis_size("sp") - 1
    kv = k_ref.shape[1] // HEAD
    sharing = q_ref.shape[1] // k_ref.shape[1]
    wide = k_ref.shape[1]

    def turn(m, low):
        m = m.astype(F32)
        half = HEAD // 2
        other = jnp.concatenate([m[:, half:], m[:, :half]], axis=1)
        high = low + m.shape[0]
        return (m * cos_ref[low:high, :] + other * sin_ref[low:high, :]).astype(BF16)

    within = lax.broadcasted_iota(jnp.int32, (rows, 3 * rows), 0)
    across = lax.broadcasted_iota(jnp.int32, (rows, 3 * rows), 1)
    far = across - rows - within
    allowed = (far <= WINDOW) & (far >= -WINDOW)
    allowed = allowed & ((across >= rows) | (me > 0))
    allowed = allowed & ((across < 2 * rows) | (me < last))
    even = (me & 1) == 0
    for g in range(kv):
        at = g * HEAD
        near = [
            (pair_ref[:, a : a + HEAD].astype(F32), outer_ref[:, a : a + HEAD].astype(F32))
            for a in (at, wide + at)
        ]
        before = [jnp.where(even, o, p) for p, o in near]
        after = [jnp.where(even, p, o) for p, o in near]
        keys = jnp.concatenate(
            [
                turn(before[0], 0),
                turn(k_ref[:, at : at + HEAD], rows),
                turn(after[0], 2 * rows),
            ],
            axis=0,
        )
        values = jnp.concatenate(
            [
                before[1].astype(BF16),
                v_ref[:, at : at + HEAD],
                after[1].astype(BF16),
            ],
            axis=0,
        )
        for j in range(sharing):
            h = g * sharing + j
            query = turn(q_ref[:, h * HEAD : (h + 1) * HEAD], rows)
            scores = nt(query, keys) * HEAD ** (-0.5)
            scores = jnp.where(allowed, scores, -jnp.inf)
            top = jnp.maximum(jnp.max(scores, axis=1, keepdims=True), sink[h])
            weights = jnp.exp(scores - top)
            total = jnp.sum(weights, axis=1, keepdims=True) + jnp.exp(sink[h] - top)
            chance = (weights / total).astype(BF16)
            out_ref[:, h * HEAD : (h + 1) * HEAD] = nn(chance, values).astype(BF16)


def finish_kernel(y_ref, read_ref, expl_ref, own_ref, got_ref, gate_ref, gain_ref, out_ref):
    _, cols = y_ref.shape
    core = lax.axis_index("sp") & 1
    wide = read_ref.shape[1]
    heads = cols // SSD_HEAD
    groups = wide // STATE
    size = cols // groups
    half = cols // 2
    spread = head_spread(heads, cols).astype(BF16)
    spread = jnp.concatenate([spread, spread], axis=0)
    for g in range(groups):
        at = g * size
        rg = read_ref[:, g * STATE : (g + 1) * STATE]
        pieces = []
        for low in range(at, at + size, min(size, half)):
            span = min(size, half)
            side = low // half
            off = low - side * half
            mine = core == side
            pieces.append(
                jnp.where(
                    mine,
                    own_ref[:, off : off + span].astype(F32),
                    got_ref[:, off : off + span].astype(F32),
                ).astype(BF16)
            )
        states = pieces[0] if len(pieces) == 1 else jnp.concatenate(pieces, axis=1)
        local = spread[:, at : at + size]
        fade_f = nn(expl_ref[:, 0 : 2 * heads], local)
        fade_b = nn(expl_ref[:, 2 * heads : 4 * heads], local)
        both = (
            y_ref[:, at : at + size]
            + fade_f * nn(rg, states[0:STATE])
            + fade_b * nn(rg, states[STATE : 2 * STATE])
        )
        gated = both * silu(gate_ref[:, at : at + size].astype(F32))
        mean = jnp.sum(gated * gated, axis=1, keepdims=True) * (1.0 / size)
        out_ref[:, at : at + size] = (
            gated * lax.rsqrt(mean + EPSILON) * gain_ref[:, at : at + size]
        ).astype(BF16)


def first_kernel(count, *refs):
    lefts = refs[: count[0]]
    shards = refs[count[0] : count[0] + count[1]]
    out_ref = refs[-1]
    left = jnp.concatenate([a[...] for a in lefts], axis=0)
    at = 0
    for shard in shards:
        span = shard.shape[1]
        out_ref[:, at : at + span] = nn(left, shard[...])
        at += span


def second_kernel(count, base, sum_ref, *refs):
    place = lax.axis_index("tp")
    blocks, shards = count
    lefts = refs[:blocks]
    pieces = refs[blocks : blocks + 2 * shards]
    outs = refs[blocks + 2 * shards : -3]
    held, early, sems = refs[-3:]
    rows = lefts[0].shape[0]
    half = rows // 2
    deep, span = pieces[0].shape
    whole = deep + pieces[shards].shape[0]
    copies = []
    for j in range(shards):
        for k in range(2):
            i = 2 * j + k
            copies.append(
                pltpu.make_async_copy(
                    pieces[k * shards + j],
                    held.at[j, 0:deep] if k == 0 else held.at[j, deep:whole],
                    sems.at[i],
                )
            )
        at = j * span
        copies.append(
            pltpu.make_async_copy(
                sum_ref.at[:, base + at : base + at + span], early.at[j], sems.at[2 * shards + j]
            )
        )
    for copy in copies:
        copy.start()
    left = jnp.concatenate([a[...] for a in lefts], axis=0)
    for j in range(shards):
        at = j * span
        for copy in copies[3 * j : 3 * j + 3]:
            copy.wait()
        total = early[j] + nn(left, held[j])
        for i in range(blocks):
            top = total[i * rows : i * rows + half]
            low = total[i * rows + half : (i + 1) * rows]
            outs[2 * i][:, at : at + span] = jnp.where(place == 0, top, low).astype(BF16)
            outs[2 * i + 1][:, at : at + span] = jnp.where(place == 0, low, top).astype(BF16)


def place_kernel(group, parts, span, *refs):
    me = lax.axis_index("sp")
    out_ref = refs[-1]
    at = 0
    for masks in parts:
        for block in group:
            for j, mask in enumerate(masks):
                low = j * span
                to = pl.multiple_of((me ^ (block ^ mask)) * span, span)
                out_ref[:, pl.ds(to, span)] = (
                    refs[at][:, low : low + span].astype(F32)
                    + refs[at + 1][:, low : low + span].astype(F32)
                ).astype(BF16)
            at += 2


def join_kernel(keep_ref, got_ref, out_ref):
    even = (lax.axis_index("sp") & 1) == 0
    end = 2 * STATE

    def load(low, high):
        mine = keep_ref[low:high, :].astype(F32)
        theirs = got_ref[low:high, :].astype(F32)
        return jnp.where(even, mine, theirs), jnp.where(even, theirs, mine)

    low, high = load(end, end + EDGE)
    low = low[0:2] + low[2:4]
    high = high[0:2] + high[2:4]
    fades = low * high
    top = fades.astype(BF16).astype(F32)
    rest = fades - top
    out_ref[end : end + EDGE, :] = jnp.concatenate(
        [top, rest, jnp.zeros((EDGE - 4, top.shape[1]), F32)], axis=0
    ).astype(BF16)
    a, b = load(0, STATE)
    out_ref[0:STATE, :] = (a * high[0:1] + b).astype(BF16)
    a, b = load(STATE, end)
    out_ref[STATE:end, :] = (b * low[1:2] + a).astype(BF16)


def flip(a, count, mask):
    return lax.ppermute(a, "sp", [(i, i ^ mask) for i in range(count)])


def outer(a, count):
    pairs = [(i, i + 1) for i in range(1, count - 1, 2)]
    return lax.ppermute(a, "sp", pairs + [(j, i) for i, j in pairs])


def cross(a, count, mask):
    return lax.ppermute(
        a,
        ("sp", "tp"),
        [(2 * i + j, 2 * (i ^ mask) + 1 - j) for i in range(count) for j in range(2)],
    )


def join_pair(keep, got):
    (payload,) = call(
        join_kernel, [jax.ShapeDtypeStruct(keep.shape, BF16)], [keep, got], flops=10**6
    )
    return payload


def tails(ref):
    end = 2 * STATE
    tail = ref[end : end + EDGE, :].astype(F32)
    return tail[0:2] + tail[2:4]


def merge_kernel(bit, first, closing, *refs):
    me = lax.axis_index("sp")
    upper = (me & bit) != 0
    end = 2 * STATE
    own_ref, other_ref = refs[0], refs[1]
    carry_ref = None if first else refs[2]
    out_ref, next_ref = refs[-2:]
    mine, theirs = tails(own_ref), tails(other_ref)
    own_f, own_b = own_ref[0:STATE, :].astype(F32), own_ref[STATE:end, :].astype(F32)
    far_f, far_b = other_ref[0:STATE, :].astype(F32), other_ref[STATE:end, :].astype(F32)
    zero = jnp.zeros_like(own_f)
    if first:
        gap_f = gap_b = jnp.ones_like(mine[0:1])
        next_ref[0:STATE, :] = jnp.where(upper, far_f, zero)
        next_ref[STATE:end, :] = jnp.where(upper, zero, far_b)
    else:
        gap_f = carry_ref[end : end + 1, :]
        gap_b = carry_ref[end + 1 : end + 2, :]
        next_ref[0:STATE, :] = carry_ref[0:STATE, :] + jnp.where(upper, far_f * gap_f, zero)
        next_ref[STATE:end, :] = carry_ref[STATE:end, :] + jnp.where(upper, zero, far_b * gap_b)
    gap_f = jnp.where(upper, gap_f * theirs[0:1], gap_f)
    gap_b = jnp.where(upper, gap_b, gap_b * theirs[1:2])
    pad = jnp.zeros((6, gap_f.shape[1]), F32)
    next_ref[end : end + 8, :] = jnp.concatenate([gap_f, gap_b, pad], axis=0)
    low_f, high_f = jnp.where(upper, far_f, own_f), jnp.where(upper, own_f, far_f)
    low_b, high_b = jnp.where(upper, far_b, own_b), jnp.where(upper, own_b, far_b)
    low, high = jnp.where(upper, theirs, mine), jnp.where(upper, mine, theirs)
    total_f = low_f * high[0:1] + high_f
    total_b = high_b * low[1:2] + low_b
    if closing:
        out_ref[...] = jnp.where((me & (2 * bit)) != 0, total_b, total_f).astype(BF16)
        return
    out_ref[0:STATE, :] = total_f.astype(BF16)
    out_ref[STATE:end, :] = total_b.astype(BF16)
    fades = low * high
    top = fades.astype(BF16).astype(F32)
    pad = jnp.zeros((EDGE - 4, fades.shape[1]), F32)
    out_ref[end : end + EDGE, :] = jnp.concatenate([top, fades - top, pad], axis=0).astype(BF16)


def close_kernel(bit, other_ref, carry_ref, keep_ref, got_ref, own_ref, away_ref):
    me = lax.axis_index("sp")
    upper = (me & bit) != 0
    even = (me & 1) == 0
    end = 2 * STATE
    other = other_ref[...].astype(F32)
    zero = jnp.zeros_like(other)
    gap_f = carry_ref[end : end + 1, :]
    gap_b = carry_ref[end + 1 : end + 2, :]
    into_f = carry_ref[0:STATE, :] + jnp.where(upper, other * gap_f, zero)
    into_b = carry_ref[STATE:end, :] + jnp.where(upper, zero, other * gap_b)
    mine, theirs = tails(keep_ref), tails(got_ref)
    keep_f, keep_b = keep_ref[0:STATE, :].astype(F32), keep_ref[STATE:end, :].astype(F32)
    got_f, got_b = got_ref[0:STATE, :].astype(F32), got_ref[STATE:end, :].astype(F32)
    low_f = jnp.where(even, keep_f, got_f)
    high_b = jnp.where(even, got_b, keep_b)
    low, high = jnp.where(even, mine, theirs), jnp.where(even, theirs, mine)
    second_f = into_f * low[0:1] + low_f
    first_b = into_b * high[1:2] + high_b
    own_ref[0:STATE, :] = jnp.where(even, into_f, second_f).astype(BF16)
    own_ref[STATE:end, :] = jnp.where(even, first_b, into_b).astype(BF16)
    away_ref[0:STATE, :] = jnp.where(even, second_f, into_f).astype(BF16)
    away_ref[STATE:end, :] = jnp.where(even, into_b, first_b).astype(BF16)


def exchange_states(keep, send, count):
    half = keep.shape[1]
    sds = jax.ShapeDtypeStruct
    got = flip(send, count, 1)
    seen = payload = join_pair(keep, got)
    carry = None
    bit = 2
    while 2 * bit < count:
        other = flip(payload, count, bit)
        closing = 4 * bit >= count
        payload, carry = call(
            functools.partial(merge_kernel, bit, carry is None, closing),
            [
                sds((STATE, half) if closing else keep.shape, BF16),
                sds((2 * STATE + 8, half), F32),
            ],
            [payload, other] + ([] if carry is None else [carry]),
            flops=10**6,
        )
        bit *= 2
    other = flip(payload, count, bit)
    own, away = call(
        functools.partial(close_kernel, bit),
        [sds((2 * STATE, half), BF16)] * 2,
        [other, carry, keep, got],
        flops=10**6,
    )
    return own, flip(away, count, 1), seen


def local(
    asking_matrix,
    matching_key_matrix,
    carried_value_matrix,
    silu_switch_argument,
    duality_source_matrix,
    storing_direction_matrix,
    fetching_direction_matrix,
    duality_kernel_coefficients,
    storing_kernel_coefficients,
    fetching_kernel_coefficients,
    raw_increment_lengths,
    logarithmic_fading_speeds,
    token_fading_spikes,
    absorber_score_vector,
    cluster_scaling_factor,
    final_mapping_matrix,
):
    rows = asking_matrix.shape[0]
    me = lax.axis_index("sp")
    count = lax.axis_size("sp")
    tps = lax.axis_size("tp")
    cols = duality_source_matrix.shape[1]
    wide = storing_direction_matrix.shape[1]
    heads = cols // SSD_HEAD
    sds = jax.ShapeDtypeStruct

    raw = (duality_source_matrix, storing_direction_matrix, fetching_direction_matrix)
    tail = jnp.concatenate([a[rows - EDGE :] for a in raw], axis=1)
    lead = jnp.concatenate([a[:EDGE] for a in raw], axis=1)
    even = (me & 1) == 0
    to_pair = jnp.where(even, tail, lead)
    to_outer = jnp.where(even, lead, tail)
    pair_edge = flip(to_pair, count, 1)
    outer_edge = outer(to_outer, count)

    span = final_mapping_matrix.shape[2]
    fast = tps == 2 and span % 128 == 0 and count == 16
    shared = [1, 4] if fast else [1]
    bits = []
    bit = count // 2
    while bit >= 2:
        if bit not in shared:
            bits.append(bit)
        bit //= 2

    def turns(a):
        got = []
        for turn in range(2):
            pairs = [(i, i ^ 8) for i in range(count) if ((i >> 2) & 1) == turn]
            got.append(lax.ppermute(a, "sp", pairs))
        return jnp.where((me & 4) == 0, got[0], got[1])

    def gather(part, piece):
        shards = {0: piece}
        for bit in bits:
            for mask in list(shards):
                if fast and bit == 8 and part in STAGGERED:
                    shards[mask ^ bit] = turns(shards[mask])
                else:
                    shards[mask ^ bit] = flip(shards[mask], count, bit)
        return shards

    deepest = final_mapping_matrix.shape[1]
    middle = deepest - deepest // LATE
    halves = [gather(0, final_mapping_matrix[0]), gather(1, final_mapping_matrix[1, :middle])]
    masks = sorted(halves[0])

    keep, send, read, inner, expl = call(
        block_kernel,
        [
            sds((2 * STATE + EDGE, cols // 2), BF16),
            sds((2 * STATE + EDGE, cols // 2), BF16),
            sds((rows, wide), BF16),
            sds((rows, cols), F32),
            sds((rows, 4 * heads), BF16),
        ],
        [
            *raw,
            pair_edge,
            outer_edge,
            duality_kernel_coefficients,
            storing_kernel_coefficients,
            fetching_kernel_coefficients,
            raw_increment_lengths.reshape(2 * heads, rows),
            logarithmic_fading_speeds,
            token_fading_spikes.reshape(2 * heads, rows),
        ],
        flops=4 * 10**9,
        scratch=[
            pltpu.VMEM((rows + 2 * EDGE, max(cols, wide)), F32),
            pltpu.VMEM((rows, cols), BF16),
            pltpu.VMEM((rows, wide), BF16),
        ],
    )
    own_state, got_state, seen = exchange_states(keep, send, count)
    later, weights, _, _ = lax.optimization_barrier(
        (me, final_mapping_matrix, matching_key_matrix, carried_value_matrix, seen)
    )[:4]
    halves.append(gather(2, weights[1, middle:]))
    pairs = jnp.concatenate([matching_key_matrix, carried_value_matrix], axis=1)
    pair_kv = flip(pairs, count, 1)
    outer_kv = outer(pairs, count)

    halfway = HEAD // 2
    spacing = ROTARY_BASE ** (-jnp.arange(halfway, dtype=F32) * 2.0 / HEAD)
    places = ((later - 1) * rows + jnp.arange(3 * rows, dtype=jnp.int32)).astype(F32)
    angles = places[:, None] * spacing[None, :]
    cosine = jnp.cos(angles)
    sine = jnp.sin(angles)
    cosine = jnp.concatenate([cosine, cosine], axis=1)
    sine = jnp.concatenate([-sine, sine], axis=1)
    (attended,) = call(
        attend_kernel,
        [sds(asking_matrix.shape, BF16)],
        [
            absorber_score_vector,
            asking_matrix,
            matching_key_matrix,
            carried_value_matrix,
            pair_kv,
            outer_kv,
            cosine,
            sine,
        ],
        flops=3 * 10**9,
        scalars=1,
    )

    def spread_rows(a):
        blocks = [a]
        for bit in reversed(shared):
            blocks += [flip(b, count, bit) for b in blocks]
        return blocks

    attended_blocks = spread_rows(attended)

    (normed,) = call(
        finish_kernel,
        [sds((rows, cols), BF16)],
        [
            inner,
            read,
            expl,
            own_state,
            got_state,
            silu_switch_argument,
            cluster_scaling_factor.reshape(1, cols),
        ],
        flops=3 * 10**9,
    )
    normed_blocks = spread_rows(normed)
    if fast:
        group = [0, 4, 1, 5]
        width = span * len(masks)
        sizes = (len(group), len(masks))
        flops = 2 * len(group) * rows * cols * width
        (early,) = call(
            functools.partial(first_kernel, sizes),
            [sds((len(group) * rows, width), F32)],
            [*attended_blocks, *[halves[0][m] for m in masks]],
            flops=flops,
        )
        pieces = []
        cut = len(masks) // PARTS
        parted = [masks[i : i + cut] for i in range(0, len(masks), cut)]
        for turn, chosen in enumerate(parted):
            wide_part = span * len(chosen)
            parts = [halves[1][m] for m in chosen] + [halves[2][m] for m in chosen]
            anywhere = pl.BlockSpec(memory_space=pl.ANY)
            deep = parts[0].shape[0] + parts[-1].shape[0]
            outs = pl.pallas_call(
                functools.partial(second_kernel, (len(group), len(chosen)), turn * cut * span),
                out_shape=[sds((rows // 2, wide_part), BF16)] * (2 * len(group)),
                in_specs=[anywhere] + [VMEM] * len(group) + [anywhere] * len(parts),
                out_specs=[VMEM] * (2 * len(group)),
                scratch_shapes=[
                    pltpu.VMEM((len(chosen), deep, span), BF16),
                    pltpu.VMEM((len(chosen), len(group) * rows, span), F32),
                    pltpu.SemaphoreType.DMA((len(parts) + len(chosen),)),
                ],
                cost_estimate=pl.CostEstimate(
                    flops=flops // PARTS, bytes_accessed=6 * 2**20, transcendentals=0
                ),
                compiler_params=pltpu.CompilerParams(vmem_limit_bytes=LIMIT),
                name="second",
            )(early, *normed_blocks, *parts)
            for i, m in enumerate(group):
                kept, gone = outs[2 * i], outs[2 * i + 1]
                pieces.append(kept if m == 0 else flip(kept, count, m))
                pieces.append(cross(gone, count, m))
        (out,) = call(
            functools.partial(place_kernel, group, parted, span),
            [sds((rows // 2, span * count), BF16)],
            pieces,
            flops=10**6,
        )
        return out

    attended_pair = attended_blocks[1]
    normed_pair = normed_blocks[1]
    shards = {
        m: jnp.stack([halves[0][m], jnp.concatenate([halves[1][m], halves[2][m]])]) for m in masks
    }
    left = jnp.concatenate(
        [
            jnp.concatenate([attended, normed], axis=1),
            jnp.concatenate([attended_pair, normed_pair], axis=1),
        ],
        axis=0,
    )
    stacked = jnp.concatenate([shards[m] for m in masks], axis=2).reshape(
        -1, span * len(masks)
    )
    partial = jnp.dot(left, stacked, preferred_element_type=F32).astype(BF16)
    partial = partial.reshape(2, tps, rows // tps, -1)
    summed = lax.psum_scatter(partial, "tp", scatter_dimension=1, tiled=True)
    summed = summed.reshape(2, rows // tps, len(masks), span)
    own, away = summed[0], flip(summed[1], count, 1)
    full = [None] * count
    for j, m in enumerate(masks):
        full[m] = own[:, j]
        full[m ^ 1] = away[:, j]
    full = jnp.stack(full, axis=0)
    bit = 1
    while bit < count:
        seen = full.reshape(count // (2 * bit), 2, bit, rows // tps, span)
        full = jnp.where((me & bit) != 0, seen[:, ::-1], seen).reshape(full.shape)
        bit *= 2
    return jnp.moveaxis(full, 0, 1).reshape(rows // tps, count * span)


def solution(mesh):
    in_specs = (
        P("sp", "tp"),
        P("sp", "tp"),
        P("sp", "tp"),
        P("sp", "tp"),
        P("sp", "tp"),
        P("sp", "tp"),
        P("sp", "tp"),
        P(None, "tp"),
        P(None, "tp"),
        P(None, "tp"),
        P(None, "tp", "sp"),
        P(None, "tp"),
        P(None, "tp", "sp"),
        P("tp"),
        P("tp"),
        P(None, "tp", "sp"),
    )
    out_specs = P(("sp", "tp"), None)

    return jax.shard_map(local, mesh=mesh, in_specs=in_specs, out_specs=out_specs, check_vma=False)
```
